32 devices in a mesh: fs: 8 (over z, x), tp: 4 (over y, core).
Axes of the slice: x: 2, y: 2, z: 4, core: 2. Of those that a mesh axis runs over, the one named last changes fastest.
Arguments:
- inputs: bfloat16 [1024, 2048], P('fs', 'tp'), may hold values from -6 to 6
- query_grad: bfloat16 [1024, 1024], P('fs', 'tp'), may hold values from -6 to 6
- forget_grad: bfloat16 [1024, 1024], P('fs', 'tp'), may hold values from -6 to 6
- forget_pre: bfloat16 [1024, 1024], P('fs', 'tp'), may hold values from -8 to 8
- lower_bound: float32 [1024], P('tp'), may hold values from 0.1 to 0.9
- query_weight: float32 [2048, 1024], P('fs', 'tp'), may hold values from -0.125 to 0.125
- forget_weight: float32 [2048, 1024], P('fs', 'tp'), may hold values from -0.125 to 0.125
- query_moment: float32 [2048, 1024], P('fs', 'tp'), may hold values from -6 to 6
- forget_moment: float32 [2048, 1024], P('fs', 'tp'), may hold values from -6 to 6
- query_rows: float32 [2048, 2048], P('fs'), may hold values from -0.6 to 0.6
- forget_rows: float32 [2048, 2048], P('fs'), may hold values from -0.6 to 0.6
- query_cols: float32 [8, 128, 128], P('tp'), may hold values from -0.6 to 0.6
- forget_cols: float32 [8, 128, 128], P('tp'), may hold values from -0.6 to 0.6
- query_row_root: bfloat16 [2048, 2048], P('fs'), may hold values from -2 to 2, as said below
- forget_row_root: bfloat16 [2048, 2048], P('fs'), may hold values from -2 to 2, as said below
- query_col_root: bfloat16 [8, 128, 128], P('tp'), may hold values from -2 to 2, as said below
- forget_col_root: bfloat16 [8, 128, 128], P('tp'), may hold values from -2 to 2, as said below
Outputs:
- query_master: float32 [2048, 1024], P('fs', 'tp')
- forget_master: float32 [2048, 1024], P('fs', 'tp')
- query_copy: bfloat16 [2048, 1024], P('fs', 'tp')
- forget_copy: bfloat16 [2048, 1024], P('fs', 'tp')
- query_step: float32 [2048, 1024], P('fs', 'tp')
- forget_step: float32 [2048, 1024], P('fs', 'tp')
- query_moment_next: float32 [2048, 1024], P('fs', 'tp')
- forget_moment_next: float32 [2048, 1024], P('fs', 'tp')
- query_rows_next: float32 [2048, 2048], P('fs')
- forget_rows_next: float32 [2048, 2048], P('fs')
- query_cols_next: float32 [8, 128, 128], P('tp')
- forget_cols_next: float32 [8, 128, 128], P('tp')
The draws below stay inside these ranges and needn't reach their ends.
Inputs may be any that keep to these rules, and one draw needn't show every extreme that they name: `query_row_root`: diagonal entries 0.5 to 1.5, the others of order 2048 ** -0.5. `forget_row_root`: diagonal entries 0.5 to 1.5, the others of order 2048 ** -0.5. `query_col_root`: diagonal entries 0.5 to 1.5, the others of order 128 ** -0.5. `forget_col_root`: diagonal entries 0.5 to 1.5, the others of order 128 ** -0.5.
All inputs are finite; a program needn't handle non-finite values.
Results may differ from the reference program's by a relative error of at most 0.005.
Values may be sent and summed in bfloat16 or wider, within the bound.
A program may use at most 64 MiB of HBM per device.

```python
import jax
import jax.numpy as jnp
from jax import lax

D = 2048
HW = 1024
HEAD = 128
TOKENS = 1024
HEADS = 8


def root_matrix(key, shape):
    order = shape[-1]
    diag_key, spread_key = jax.random.split(key)
    spread = jnp.clip(jax.random.normal(spread_key, shape, jnp.float32), -4.0, 4.0) * order ** (-0.5)
    diagonal = jax.random.uniform(diag_key, shape[:-1], jnp.float32, 0.5, 1.5)
    unit_eye = jnp.eye(order, dtype=jnp.float32)
    return (spread * (1.0 - unit_eye) + diagonal[..., None] * unit_eye).astype(jnp.bfloat16)


def draw_query_row_root(key, part):
    return root_matrix(jax.random.fold_in(key, 11), (D, D))


def draw_forget_row_root(key, part):
    return root_matrix(jax.random.fold_in(key, 23), (D, D))


def draw_query_col_root(key, part):
    return root_matrix(jax.random.fold_in(key, 37), (HEADS, HEAD, HEAD))


def draw_forget_col_root(key, part):
    return root_matrix(jax.random.fold_in(key, 41), (HEADS, HEAD, HEAD))


def raised(entries, own_key, source, target, parts, factor):
    owner, partner = [(jnp.arange(entries.shape[dim]) // (entries.shape[dim] // parts)).reshape([-1 if axis == dim else 1 for axis in range(entries.ndim)]) for dim in (source, target)]
    chosen = jax.random.permutation(own_key, parts)[partner]
    strong = (owner == chosen) | (owner == (partner + parts // 2) % parts)
    return jnp.where(strong, factor * entries, entries)


def steps_of(rng, shape, shards, low, high):
    factor_of, own = 1.0, jax.random.fold_in(rng, 6)
    for dim, shards_of in shards:
        steps = jnp.exp(jax.random.uniform(jax.random.fold_in(own, dim), (shards_of,), jnp.float32, low / len(shards), high / len(shards)))
        factor_of = factor_of * jnp.repeat(steps, shape[dim] // shards_of).reshape([-1 if axis == dim else 1 for axis in range(len(shape))])
    return factor_of


def gaussian(rng, extent, deviation, bound, cuts=(), kind=jnp.bfloat16):
    array = jax.random.normal(rng, extent, jnp.float32) * deviation
    if len(cuts) > 0:
        array = steps_of(rng, extent, cuts, -0.22, 0.18) * array
    return jnp.clip(array, min=-bound, max=bound).astype(kind)


def bell_draw_with(key, extent, deviation, limit, shards, heavy, held_as=jnp.bfloat16):
    drawn = deviation * jax.random.normal(key, extent, jnp.float32)
    if shards:
        drawn = drawn * steps_of(key, extent, shards, -0.22, 0.18)
    return jnp.clip(raised(drawn, jax.random.fold_in(key, 3), *heavy), -limit, limit).astype(held_as)


def setup_inputs(seed: int = 0) -> dict:
    key_list = jax.random.split(jax.random.key(seed), 18)
    inputs = bell_draw_with(key_list[0], (TOKENS, D), 1.0, 6.0, ((0, 8), (1, 4)), (0, 1, 8, 2.0))
    query_grad = gaussian(key_list[1], (TOKENS, HW), 1.0, 6.0, ((0, 8), (1, 4)))
    forget_grad = gaussian(key_list[2], (TOKENS, HW), 1.0, 6.0, ((0, 8), (1, 4)))
    forget_pre = gaussian(key_list[3], (TOKENS, HW), 2.0, 8.0, ((0, 8), (1, 4)))
    lower_bound = jnp.clip(0.1 + 0.79999997 * jax.random.uniform(key_list[4], (HW,), jnp.float32) ** steps_of(key_list[4], (HW,), ((0, 4),), -0.2, 0.2), 0.1, 0.9)
    query_weight = gaussian(key_list[5], (D, HW), D ** -0.5, 0.125, ((0, 8), (1, 4)), jnp.float32)
    forget_weight = gaussian(key_list[6], (D, HW), D ** -0.5, 0.125, ((0, 8), (1, 4)), jnp.float32)
    query_moment = gaussian(key_list[7], (D, HW), 1.0, 6.0, ((0, 8), (1, 4)), jnp.float32)
    forget_moment = gaussian(key_list[8], (D, HW), 1.0, 6.0, ((0, 8), (1, 4)), jnp.float32)
    query_rows = gaussian(key_list[9], (D, D), 0.1, 0.6, ((0, 8),), jnp.float32)
    forget_rows = gaussian(key_list[10], (D, D), 0.1, 0.6, ((0, 8),), jnp.float32)
    query_cols = gaussian(key_list[11], (HEADS, HEAD, HEAD), 0.1, 0.6, ((0, 4),), jnp.float32)
    forget_cols = gaussian(key_list[12], (HEADS, HEAD, HEAD), 0.1, 0.6, ((0, 4),), jnp.float32)
    query_row_root = draw_query_row_root(jax.random.fold_in(key_list[17], 71), 0)
    forget_row_root = draw_forget_row_root(jax.random.fold_in(key_list[17], 71), 0)
    query_col_root = draw_query_col_root(jax.random.fold_in(key_list[17], 71), 0)
    forget_col_root = draw_forget_col_root(jax.random.fold_in(key_list[17], 71), 0)
    return dict(inputs=inputs, query_grad=query_grad, forget_grad=forget_grad, forget_pre=forget_pre, lower_bound=lower_bound, query_weight=query_weight, forget_weight=forget_weight, query_moment=query_moment, forget_moment=forget_moment, query_rows=query_rows, forget_rows=forget_rows, query_cols=query_cols, forget_cols=forget_cols, query_row_root=query_row_root, forget_row_root=forget_row_root, query_col_root=query_col_root, forget_col_root=forget_col_root)


stat_decay = 0.9
moment_decay = 0.9
learn_rate = 0.02
highest = lax.Precision.HIGHEST

def finish(gradient, weight, moment, rows, cols, row_root, col_root):
    square = jnp.sum(gradient * gradient)
    norm_scale = jnp.sqrt(D * HW / (square + 1.0))
    scaled = gradient * norm_scale
    rows_next = stat_decay * rows + (1.0 - stat_decay) / HW * jnp.dot(scaled, scaled.T, precision=highest)
    by_head = scaled.reshape(D, HEADS, HEAD)
    cols_next = stat_decay * cols + (1.0 - stat_decay) / D * jnp.einsum('rhi,rhj->hij', by_head, by_head, precision=highest)
    left_sum = jnp.dot(row_root.astype(jnp.float32), gradient, precision=highest)
    precond = norm_scale * jnp.einsum('rhi,hij->rhj', left_sum.reshape(D, HEADS, HEAD), col_root.astype(jnp.float32), precision=highest).reshape(D, HW)
    moment_next = moment_decay * moment + (1.0 - moment_decay) * precond
    update_step = moment_decay * moment_next + (1.0 - moment_decay) * precond
    master = weight - learn_rate * update_step
    return (master, master.astype(jnp.bfloat16), update_step, moment_next, rows_next, cols_next)

def reference(inputs, query_grad, forget_grad, forget_pre, lower_bound, query_weight, forget_weight, query_moment, forget_moment, query_rows, forget_rows, query_cols, forget_cols, query_row_root, forget_row_root, query_col_root, forget_col_root):
    sigma_gate = jax.nn.sigmoid(forget_pre.astype(jnp.float32))
    forget_cot = (forget_grad.astype(jnp.float32) * (1.0 - lower_bound) * sigma_gate * (1.0 - sigma_gate)).astype(jnp.bfloat16)
    query_gradient = jnp.dot(inputs.T, query_grad, preferred_element_type=jnp.float32)
    forget_gradient = jnp.dot(inputs.T, forget_cot, preferred_element_type=jnp.float32)
    query_out = finish(query_gradient, query_weight, query_moment, query_rows, query_cols, query_row_root, query_col_root)
    forget_out = finish(forget_gradient, forget_weight, forget_moment, forget_rows, forget_cols, forget_row_root, forget_col_root)
    return (query_out[0], forget_out[0], query_out[1], forget_out[1], query_out[2], forget_out[2], query_out[3], forget_out[3], query_out[4], forget_out[4], query_out[5], forget_out[5])
```

```python
import jax
import jax.numpy as jnp
from jax import lax
from jax.sharding import PartitionSpec as P

D = 2048
HW = 1024
HEAD = 128


stat_decay = 0.9
moment_decay = 0.9
learn_rate = 0.02
highest = lax.Precision.HIGHEST


def fold_one(carry_state, shard_piece, offset, root_mine, grad_mine):
    left_sum, outer_rows, column_total = carry_state
    row_count, col_width = shard_piece.shape
    left_sum = left_sum + jnp.dot(root_mine, shard_piece, precision=highest)
    outer_piece = lax.dot_general(
        grad_mine, shard_piece, (((1,), (1,)), ((), ())), precision=highest
    )
    outer_rows = lax.dynamic_update_slice_in_dim(outer_rows, outer_piece, offset, 1)
    by_head = shard_piece.reshape(row_count, col_width // HEAD, HEAD)
    column_total = column_total + jnp.einsum("rhi,rhj->hij", by_head, by_head, precision=highest)
    return (left_sum, outer_rows, column_total)


def finish(weight, moment, rows, cols, col_root, left_sum, outer_rows, column_total, square):
    norm_scale = jnp.sqrt(D * HW / (square + 1.0))
    scale_twice = norm_scale * norm_scale
    rows_next = stat_decay * rows + (1.0 - stat_decay) / HW * scale_twice * outer_rows
    cols_next = stat_decay * cols + (1.0 - stat_decay) / D * scale_twice * column_total
    shard_rows, col_width = left_sum.shape
    shaped = left_sum.reshape(shard_rows, col_width // HEAD, HEAD)
    precond = norm_scale * jnp.einsum(
        "rhi,hij->rhj", shaped, col_root.astype(jnp.float32), precision=highest
    ).reshape(shard_rows, col_width)
    moment_next = moment_decay * moment + (1.0 - moment_decay) * precond
    update_step = moment_decay * moment_next + (1.0 - moment_decay) * precond
    master = weight - learn_rate * update_step
    return (master, master.astype(jnp.bfloat16), update_step, moment_next, rows_next, cols_next)


def reduce_plan(
    inputs,
    query_grad,
    forget_grad,
    forget_pre,
    lower_bound,
    query_weight,
    forget_weight,
    query_moment,
    forget_moment,
    query_rows,
    forget_rows,
    query_cols,
    forget_cols,
    query_row_root,
    forget_row_root,
    query_col_root,
    forget_col_root,
):
    sigma_gate = jax.nn.sigmoid(forget_pre.astype(jnp.float32))
    forget_cot = (
        forget_grad.astype(jnp.float32) * (1.0 - lower_bound) * sigma_gate * (1.0 - sigma_gate)
    ).astype(jnp.bfloat16)
    gathered = lax.all_gather(inputs, "tp", axis=1, tiled=True)
    shard_rows, col_width = query_weight.shape
    heads_here = col_width // HEAD
    row_roots = (query_row_root.astype(jnp.float32), forget_row_root.astype(jnp.float32))
    empty = (
        jnp.zeros((shard_rows, col_width), jnp.float32),
        jnp.zeros((shard_rows, D), jnp.float32),
        jnp.zeros((heads_here, HEAD, HEAD), jnp.float32),
    )
    joined = jnp.concatenate([query_grad, forget_cot], axis=1)
    summed = lax.psum_scatter(
        lax.dot_general(
            gathered, joined, (((0,), (0,)), ((), ())), preferred_element_type=jnp.float32
        ),
        "fs",
        scatter_dimension=0,
        tiled=True,
    )
    gradients = (summed[:, :col_width], summed[:, col_width:])
    offset = jnp.int32(0)
    results = (
        fold_one(
            empty,
            lax.all_gather(gradients[0].astype(jnp.bfloat16), "fs", axis=0, tiled=True).astype(
                jnp.float32
            ),
            offset,
            row_roots[0],
            gradients[0],
        ),
        fold_one(
            empty,
            lax.all_gather(gradients[1].astype(jnp.bfloat16), "fs", axis=0, tiled=True).astype(
                jnp.float32
            ),
            offset,
            row_roots[1],
            gradients[1],
        ),
    )
    query_trace = jnp.sum(jnp.diagonal(results[0][2], axis1=1, axis2=2))
    forget_trace = jnp.sum(jnp.diagonal(results[1][2], axis1=1, axis2=2))
    query_outer, forget_outer, query_square, forget_square = (
        lax.psum(results[0][1].astype(jnp.bfloat16), "tp").astype(jnp.float32),
        lax.psum(results[1][1].astype(jnp.bfloat16), "tp").astype(jnp.float32),
        lax.psum(query_trace.astype(jnp.bfloat16), "tp").astype(jnp.float32),
        lax.psum(forget_trace.astype(jnp.bfloat16), "tp").astype(jnp.float32),
    )
    query_out = finish(
        query_weight,
        query_moment,
        query_rows,
        query_cols,
        query_col_root,
        results[0][0],
        query_outer,
        results[0][2],
        query_square,
    )
    forget_out = finish(
        forget_weight,
        forget_moment,
        forget_rows,
        forget_cols,
        forget_col_root,
        results[1][0],
        forget_outer,
        results[1][2],
        forget_square,
    )
    return (
        query_out[0],
        forget_out[0],
        query_out[1],
        forget_out[1],
        query_out[2],
        forget_out[2],
        query_out[3],
        forget_out[3],
        query_out[4],
        forget_out[4],
        query_out[5],
        forget_out[5],
    )


def to_bf16(value):
    return value.astype(jnp.bfloat16)


def wide_dot(left, right, dims):
    return lax.dot_general(left, right, (dims, ((), ())), preferred_element_type=jnp.float32)


def gather_blocks(tokens_block, cot_block):
    axes = ("fs", "tp")
    sizes = (lax.axis_size("fs"), lax.axis_size("tp"))
    gathered = lax.all_gather(tokens_block, axes, axis=0, tiled=False)
    cots = lax.all_gather(cot_block, axes, axis=0, tiled=False)
    return (
        gathered.reshape(sizes + tokens_block.shape),
        cots.reshape(sizes + cot_block.shape),
    )


def whole(blocks):
    shards, parts, rows, cols = blocks.shape
    return blocks.transpose(0, 2, 1, 3).reshape(shards * rows, parts * cols)


def update(weight, moment, rows, cols, row_root, col_root, inputs_all, cot_all):
    gradient = wide_dot(inputs_all, cot_all, ((0,), (0,)))
    square = jnp.sum(gradient * gradient)
    norm_scale = jnp.sqrt(gradient.shape[0] * gradient.shape[1] / (square + 1.0))
    scale_twice = norm_scale * norm_scale
    narrow = to_bf16(gradient)
    shard_rows, col_width = weight.shape
    mine = lax.dynamic_slice_in_dim(narrow, lax.axis_index("fs") * shard_rows, shard_rows, 0)
    own = lax.dynamic_slice_in_dim(narrow, lax.axis_index("tp") * col_width, col_width, 1)
    outer = wide_dot(mine, narrow, ((1,), (1,)))
    rows_next = stat_decay * rows + (1.0 - stat_decay) / HW * scale_twice * outer
    heads = col_width // HEAD
    left_sum = to_bf16(wide_dot(row_root, own, ((1,), (0,))))
    column_parts = []
    precond_parts = []
    for head in range(heads):
        part = own[:, head * HEAD : (head + 1) * HEAD]
        column_parts.append(wide_dot(part, part, ((0,), (0,))))
        precond_parts.append(
            wide_dot(left_sum[:, head * HEAD : (head + 1) * HEAD], col_root[head], ((1,), (0,)))
        )
    cols_next = stat_decay * cols + (1.0 - stat_decay) / D * scale_twice * jnp.stack(column_parts)
    precond = norm_scale * jnp.concatenate(precond_parts, axis=1)
    moment_next = moment_decay * moment + (1.0 - moment_decay) * precond
    update_step = moment_decay * moment_next + (1.0 - moment_decay) * precond
    master = weight - learn_rate * update_step
    return (master, to_bf16(master), update_step, moment_next, rows_next, cols_next)


def gather_plan(
    inputs,
    query_grad,
    forget_grad,
    forget_pre,
    lower_bound,
    query_weight,
    forget_weight,
    query_moment,
    forget_moment,
    query_rows,
    forget_rows,
    query_cols,
    forget_cols,
    query_row_root,
    forget_row_root,
    query_col_root,
    forget_col_root,
):
    sigma_gate = jax.nn.sigmoid(forget_pre.astype(jnp.float32))
    forget_cot = to_bf16(
        forget_grad.astype(jnp.float32) * (1.0 - lower_bound) * sigma_gate * (1.0 - sigma_gate)
    )
    width = query_grad.shape[1]
    inputs_all, cots = gather_blocks(inputs, jnp.concatenate([query_grad, forget_cot], axis=1))
    inputs_all = whole(inputs_all)
    query_out = update(
        query_weight, query_moment, query_rows, query_cols, query_row_root, query_col_root,
        inputs_all, whole(cots[..., :width]),
    )
    forget_out = update(
        forget_weight, forget_moment, forget_rows, forget_cols, forget_row_root, forget_col_root,
        inputs_all, whole(cots[..., width:]),
    )
    return tuple(piece for pair in zip(query_out, forget_out) for piece in pair)


def on_device(*args):
    token_count = args[0].shape[0] * lax.axis_size("fs")
    feature_count = args[0].shape[1] * lax.axis_size("tp")
    if token_count <= feature_count:
        return gather_plan(*args)
    return reduce_plan(*args)


def solution(mesh):
    in_specs = (
        P("fs", "tp"),
        P("fs", "tp"),
        P("fs", "tp"),
        P("fs", "tp"),
        P("tp"),
        P("fs", "tp"),
        P("fs", "tp"),
        P("fs", "tp"),
        P("fs", "tp"),
        P("fs", None),
        P("fs", None),
        P("tp", None, None),
        P("tp", None, None),
        P("fs", None),
        P("fs", None),
        P("tp", None, None),
        P("tp", None, None),
    )
    out_specs = (
        P("fs", "tp"),
        P("fs", "tp"),
        P("fs", "tp"),
        P("fs", "tp"),
        P("fs", "tp"),
        P("fs", "tp"),
        P("fs", "tp"),
        P("fs", "tp"),
        P("fs", None),
        P("fs", None),
        P("tp", None, None),
        P("tp", None, None),
    )
    return jax.shard_map(
        on_device, mesh=mesh, in_specs=in_specs, out_specs=out_specs, check_vma=False
    )
```

```python
import functools

import jax
import jax.numpy as jnp
from jax import lax
from jax.experimental import pallas as pl
from jax.experimental.pallas import tpu as pltpu
from jax.sharding import PartitionSpec as P

D = 2048
HW = 1024
HEAD = 128


stat_decay = 0.9
moment_decay = 0.9
learn_rate = 0.02
highest = lax.Precision.HIGHEST
MESH = pl.DeviceIdType.MESH


def fold_one(carry_state, shard_piece, offset, root_mine, grad_mine):
    left_sum, outer_rows, column_total = carry_state
    row_count, col_width = shard_piece.shape
    left_sum = left_sum + jnp.dot(root_mine, shard_piece, precision=highest)
    outer_piece = lax.dot_general(
        grad_mine, shard_piece, (((1,), (1,)), ((), ())), precision=highest
    )
    outer_rows = lax.dynamic_update_slice_in_dim(outer_rows, outer_piece, offset, 1)
    by_head = shard_piece.reshape(row_count, col_width // HEAD, HEAD)
    column_total = column_total + jnp.einsum("rhi,rhj->hij", by_head, by_head, precision=highest)
    return (left_sum, outer_rows, column_total)


def finish(weight, moment, rows, cols, col_root, left_sum, outer_rows, column_total, square):
    norm_scale = jnp.sqrt(D * HW / (square + 1.0))
    scale_twice = norm_scale * norm_scale
    rows_next = stat_decay * rows + (1.0 - stat_decay) / HW * scale_twice * outer_rows
    cols_next = stat_decay * cols + (1.0 - stat_decay) / D * scale_twice * column_total
    shard_rows, col_width = left_sum.shape
    shaped = left_sum.reshape(shard_rows, col_width // HEAD, HEAD)
    precond = norm_scale * jnp.einsum(
        "rhi,hij->rhj", shaped, col_root.astype(jnp.float32), precision=highest
    ).reshape(shard_rows, col_width)
    moment_next = moment_decay * moment + (1.0 - moment_decay) * precond
    update_step = moment_decay * moment_next + (1.0 - moment_decay) * precond
    master = weight - learn_rate * update_step
    return (master, master.astype(jnp.bfloat16), update_step, moment_next, rows_next, cols_next)


def reduce_plan(
    inputs,
    query_grad,
    forget_grad,
    forget_pre,
    lower_bound,
    query_weight,
    forget_weight,
    query_moment,
    forget_moment,
    query_rows,
    forget_rows,
    query_cols,
    forget_cols,
    query_row_root,
    forget_row_root,
    query_col_root,
    forget_col_root,
):
    sigma_gate = jax.nn.sigmoid(forget_pre.astype(jnp.float32))
    forget_cot = (
        forget_grad.astype(jnp.float32) * (1.0 - lower_bound) * sigma_gate * (1.0 - sigma_gate)
    ).astype(jnp.bfloat16)
    gathered = lax.all_gather(inputs, "tp", axis=1, tiled=True)
    shard_rows, col_width = query_weight.shape
    heads_here = col_width // HEAD
    row_roots = (query_row_root.astype(jnp.float32), forget_row_root.astype(jnp.float32))
    empty = (
        jnp.zeros((shard_rows, col_width), jnp.float32),
        jnp.zeros((shard_rows, D), jnp.float32),
        jnp.zeros((heads_here, HEAD, HEAD), jnp.float32),
    )
    joined = jnp.concatenate([query_grad, forget_cot], axis=1)
    summed = lax.psum_scatter(
        lax.dot_general(
            gathered, joined, (((0,), (0,)), ((), ())), preferred_element_type=jnp.float32
        ),
        "fs",
        scatter_dimension=0,
        tiled=True,
    )
    gradients = (summed[:, :col_width], summed[:, col_width:])
    offset = jnp.int32(0)
    results = (
        fold_one(
            empty,
            lax.all_gather(gradients[0].astype(jnp.bfloat16), "fs", axis=0, tiled=True).astype(
                jnp.float32
            ),
            offset,
            row_roots[0],
            gradients[0],
        ),
        fold_one(
            empty,
            lax.all_gather(gradients[1].astype(jnp.bfloat16), "fs", axis=0, tiled=True).astype(
                jnp.float32
            ),
            offset,
            row_roots[1],
            gradients[1],
        ),
    )
    query_trace = jnp.sum(jnp.diagonal(results[0][2], axis1=1, axis2=2))
    forget_trace = jnp.sum(jnp.diagonal(results[1][2], axis1=1, axis2=2))
    query_outer, forget_outer, query_square, forget_square = (
        lax.psum(results[0][1].astype(jnp.bfloat16), "tp").astype(jnp.float32),
        lax.psum(results[1][1].astype(jnp.bfloat16), "tp").astype(jnp.float32),
        lax.psum(query_trace.astype(jnp.bfloat16), "tp").astype(jnp.float32),
        lax.psum(forget_trace.astype(jnp.bfloat16), "tp").astype(jnp.float32),
    )
    query_out = finish(
        query_weight,
        query_moment,
        query_rows,
        query_cols,
        query_col_root,
        results[0][0],
        query_outer,
        results[0][2],
        query_square,
    )
    forget_out = finish(
        forget_weight,
        forget_moment,
        forget_rows,
        forget_cols,
        forget_col_root,
        results[1][0],
        forget_outer,
        results[1][2],
        forget_square,
    )
    return (
        query_out[0],
        forget_out[0],
        query_out[1],
        forget_out[1],
        query_out[2],
        forget_out[2],
        query_out[3],
        forget_out[3],
        query_out[4],
        forget_out[4],
        query_out[5],
        forget_out[5],
    )


def to_bf16(value):
    return value.astype(jnp.bfloat16)


def wide_dot(left, right, dims):
    return lax.dot_general(left, right, (dims, ((), ())), preferred_element_type=jnp.float32)


def relay_kernel(
    x_ref, g_ref, rq_ref, rf_ref, cq_ref, cf_ref,
    sq_ref, sf_ref, pq_ref, pf_ref, kq_ref, kf_ref,
    xs, gs, xt, grad, left, own_sem, send_sem, recv_sem,
):
    shards = xs.shape[0]
    depth = shards // 2
    block, span = x_ref.shape
    fs = lax.axis_index("fs")
    tp = lax.axis_index("tp")
    z, px = lax.div(fs, 2), lax.rem(fs, 2)
    py, pc = lax.div(tp, 2), lax.rem(tp, 2)
    fs_other = fs + 1 - 2 * px
    tp_other = tp + 2 - 4 * py
    beside = {
        "up": (fs + 2, tp),
        "down": (fs - 2, tp),
        "x": (fs_other, tp),
        "y": (fs, tp_other),
        "core": (fs, tp + 1 - 2 * pc),
    }
    has_up = z < depth - 1
    has_down = z > 0

    def guarded(cond, action):
        if cond is None:
            action()
        else:
            pl.when(cond)(action)

    barrier = pltpu.get_barrier_semaphore()

    def greet(name):
        pl.semaphore_signal(barrier, inc=1, device_id=beside[name], device_id_type=MESH)

    for name in ("x", "y", "core"):
        greet(name)
    guarded(has_up, lambda: greet("up"))
    guarded(has_down, lambda: greet("down"))
    pl.semaphore_wait(
        barrier, 3 + jnp.where(has_up, 1, 0) + jnp.where(has_down, 1, 0)
    )

    slots = (xs, gs)
    pending = []

    def copy_of(kind, src, slot, name, number):
        return pltpu.make_async_remote_copy(
            src_ref=src,
            dst_ref=slots[kind].at[slot[0], slot[1]],
            send_sem=send_sem.at[number],
            recv_sem=recv_sem.at[kind, slot[0], slot[1]],
            device_id=beside[name],
            device_id_type=MESH,
        )

    def send(kind, src, slot, name, cond=None):
        number = len(pending)
        build = functools.partial(copy_of, kind, src, slot, name, number)
        guarded(cond, lambda: build().start())
        pending.append((cond, build))

    def arrive(kind, slot, cond=None):
        here = slots[kind].at[slot[0], slot[1]]
        guarded(cond, lambda: copy_of(kind, here, slot, "core", 0).wait_recv())

    def forward(kind, slot, names, cond=None):
        for name in names:
            send(kind, slots[kind].at[slot[0], slot[1]], slot, name, cond)

    own = (fs, tp)
    orders = (("x", "y"), ("y", "x"))
    sources = (x_ref, g_ref)

    def crossed(kind, layer):
        if kind == 0:
            return (2 * layer + 1 - px, tp)
        return (2 * layer + px, tp_other)

    def lasts(kind, layer):
        if kind == 0:
            return ((2 * layer + px, tp_other), (2 * layer + 1 - px, tp_other))
        return ((2 * layer + 1 - px, tp), (2 * layer + 1 - px, tp_other))

    keep = [
        pltpu.make_async_copy(sources[kind], slots[kind].at[fs, tp], own_sem.at[kind])
        for kind in range(2)
    ]
    for kind in range(2):
        send(kind, sources[kind], own, "up", has_up)
        send(kind, sources[kind], own, "down", has_down)
    for kind in range(2):
        send(kind, sources[kind], own, orders[kind][0])
    for kind in range(2):
        send(kind, sources[kind], own, orders[kind][1])
        send(kind, sources[kind], own, "core")
        keep[kind].start()

    def finals(stage):
        for layer, cond in stage:
            for kind in range(2):
                for slot in lasts(kind, layer):
                    arrive(kind, slot, cond)
                    forward(kind, slot, ("core",), cond)

    previous = None
    for distance in range(depth):
        stage = []
        if distance == 0:
            stage.append((z, None))
        else:
            stage.append((z - distance, z >= distance))
            stage.append((z + distance, z + distance < depth))
            for sign, (layer, cond) in zip((-1, 1), stage):
                for kind in range(2):
                    slot = (2 * layer + px, tp)
                    arrive(kind, slot, cond)
                    if sign < 0:
                        onward, onto = "up", jnp.logical_and(cond, has_up)
                    else:
                        onward, onto = "down", jnp.logical_and(cond, has_down)
                    if distance < depth - 1:
                        forward(kind, slot, (onward,), onto)
                    forward(kind, slot, orders[kind] + ("core",), cond)
        for layer, cond in stage:
            for kind in range(2):
                slot = crossed(kind, layer)
                arrive(kind, slot, cond)
                forward(kind, slot, (orders[kind][1], "core"), cond)
        if previous is not None:
            finals(previous)
        previous = stage
    finals(previous)
    for kind in range(2):
        keep[kind].wait()
    for layer in range(depth):
        for across in range(2):
            for part in range(2):
                slot = (2 * layer + across, 2 * part + 1 - pc)
                for kind in range(2):
                    arrive(kind, slot)

    @pl.loop(0, shards)
    def _(shard):
        lanes = pl.ds(pl.multiple_of(shard * block, block), block)
        for part in range(xs.shape[1]):
            xt[part * span : (part + 1) * span, lanes] = xs[shard, part].T

    width = gs.shape[3] // 2
    chunk = sq_ref.shape[0]
    steps = xt.shape[0] // chunk
    tokens = shards * block
    own_lanes = pl.ds(pl.multiple_of(tp * width, width), width)
    for which, (root, col_root, outer_ref, pre_ref, col_ref) in enumerate(
        (
            (rq_ref, cq_ref, sq_ref, pq_ref, kq_ref),
            (rf_ref, cf_ref, sf_ref, pf_ref, kf_ref),
        )
    ):
        def multiply(step, total, which=which):
            rows = pl.ds(pl.multiple_of(step * chunk, chunk), chunk)
            for part in range(gs.shape[1]):
                cot = gs[:, part, :, which * width : (which + 1) * width].reshape(tokens, width)
                piece = wide_dot(xt[rows, :], cot, ((1,), (0,)))
                grad[rows, part * width : (part + 1) * width] = to_bf16(piece)
                total = total + jnp.sum(piece * piece, axis=0, keepdims=True)
            return total

        total = lax.fori_loop(0, steps, multiply, jnp.zeros((1, width), jnp.float32))
        square = jnp.sum(total, axis=1, keepdims=True)
        scale_twice = float(grad.shape[0] * grad.shape[1]) / (square + 1.0)
        norm_scale = jnp.sqrt(scale_twice)
        left[...] = jnp.zeros_like(left)
        col_ref[...] = jnp.zeros_like(col_ref)
        mine = pl.ds(pl.multiple_of(fs * chunk, chunk), chunk)

        @pl.loop(0, steps)
        def _(step):
            rows = pl.ds(pl.multiple_of(step * chunk, chunk), chunk)
            outer = wide_dot(grad[mine, :], grad[rows, :], ((1,), (1,)))
            outer_ref[:, rows] = to_bf16(
                outer * ((1.0 - stat_decay) / grad.shape[1] * scale_twice)
            )
            part = grad[rows, own_lanes]
            left[...] += wide_dot(root[:, rows], part, ((1,), (0,)))
            for head in range(width // HEAD):
                piece = part[:, head * HEAD : (head + 1) * HEAD]
                col_ref[head] += wide_dot(piece, piece, ((0,), (0,)))

        for head in range(width // HEAD):
            lanes = slice(head * HEAD, (head + 1) * HEAD)
            col_ref[head] = col_ref[head] * ((1.0 - stat_decay) / grad.shape[0] * scale_twice)
            pre_ref[:, lanes] = norm_scale * wide_dot(
                to_bf16(left[:, lanes]), col_root[head], ((1,), (0,))
            )

    for cond, build in pending:
        guarded(cond, lambda build=build: build().wait_send())


def relayed_products(x, cots, query_root, forget_root, query_col_root, forget_col_root):
    shards, parts = lax.axis_size("fs"), lax.axis_size("tp")
    block, span = x.shape
    width = cots.shape[1] // 2
    chunk, features = query_root.shape
    depth = shards // 2
    sends = 2 * (5 + 8 * (depth - 1) + 2 * (2 * depth - 1) + 2 * (2 * depth - 1))
    f32 = jnp.float32
    heads = query_col_root.shape
    vmem = pl.BlockSpec(memory_space=pltpu.VMEM)
    return pl.pallas_call(
        relay_kernel,
        out_shape=[
            jax.ShapeDtypeStruct((chunk, features), jnp.bfloat16),
            jax.ShapeDtypeStruct((chunk, features), jnp.bfloat16),
            jax.ShapeDtypeStruct((chunk, width), f32),
            jax.ShapeDtypeStruct((chunk, width), f32),
            jax.ShapeDtypeStruct(heads, f32),
            jax.ShapeDtypeStruct(heads, f32),
        ],
        in_specs=[vmem] * 6,
        out_specs=[vmem] * 6,
        scratch_shapes=[
            pltpu.VMEM((shards, parts, block, span), jnp.bfloat16),
            pltpu.VMEM((shards, parts, block, 2 * width), jnp.bfloat16),
            pltpu.VMEM((features, shards * block), jnp.bfloat16),
            pltpu.VMEM((features, parts * width), jnp.bfloat16),
            pltpu.VMEM((chunk, width), f32),
            pltpu.SemaphoreType.DMA((2,)),
            pltpu.SemaphoreType.DMA((sends,)),
            pltpu.SemaphoreType.DMA((2, shards, parts)),
        ],
        compiler_params=pltpu.CompilerParams(
            collective_id=0, has_side_effects=True, vmem_limit_bytes=56 * 1024 * 1024
        ),
    )(x, cots, query_root, forget_root, query_col_root, forget_col_root)


def finish_update(weight, moment, rows, cols, outer, precond, column):
    rows_next = stat_decay * rows + outer.astype(jnp.float32)
    cols_next = stat_decay * cols + column
    moment_next = moment_decay * moment + (1.0 - moment_decay) * precond
    update_step = moment_decay * moment_next + (1.0 - moment_decay) * precond
    master = weight - learn_rate * update_step
    return (master, to_bf16(master), update_step, moment_next, rows_next, cols_next)


def gather_plan(
    inputs,
    query_grad,
    forget_grad,
    forget_pre,
    lower_bound,
    query_weight,
    forget_weight,
    query_moment,
    forget_moment,
    query_rows,
    forget_rows,
    query_cols,
    forget_cols,
    query_row_root,
    forget_row_root,
    query_col_root,
    forget_col_root,
):
    sigma_gate = jax.nn.sigmoid(forget_pre.astype(jnp.float32))
    forget_cot = to_bf16(
        forget_grad.astype(jnp.float32) * (1.0 - lower_bound) * sigma_gate * (1.0 - sigma_gate)
    )
    query_outer, forget_outer, query_pre, forget_pre_out, query_column, forget_column = (
        relayed_products(
            inputs,
            jnp.concatenate([query_grad, forget_cot], axis=1),
            query_row_root,
            forget_row_root,
            query_col_root,
            forget_col_root,
        )
    )
    query_out = finish_update(
        query_weight, query_moment, query_rows, query_cols, query_outer, query_pre, query_column
    )
    forget_out = finish_update(
        forget_weight, forget_moment, forget_rows, forget_cols,
        forget_outer, forget_pre_out, forget_column,
    )
    return tuple(piece for pair in zip(query_out, forget_out) for piece in pair)


def on_device(*args):
    token_count = args[0].shape[0] * lax.axis_size("fs")
    feature_count = args[0].shape[1] * lax.axis_size("tp")
    paired = lax.axis_size("fs") % 2 == 0 and lax.axis_size("tp") == 4
    if paired and token_count <= feature_count:
        return gather_plan(*args)
    return reduce_plan(*args)


def solution(mesh):
    in_specs = (
        P("fs", "tp"),
        P("fs", "tp"),
        P("fs", "tp"),
        P("fs", "tp"),
        P("tp"),
        P("fs", "tp"),
        P("fs", "tp"),
        P("fs", "tp"),
        P("fs", "tp"),
        P("fs", None),
        P("fs", None),
        P("tp", None, None),
        P("tp", None, None),
        P("fs", None),
        P("fs", None),
        P("tp", None, None),
        P("tp", None, None),
    )
    out_specs = (
        P("fs", "tp"),
        P("fs", "tp"),
        P("fs", "tp"),
        P("fs", "tp"),
        P("fs", "tp"),
        P("fs", "tp"),
        P("fs", "tp"),
        P("fs", "tp"),
        P("fs", None),
        P("fs", None),
        P("tp", None, None),
        P("tp", None, None),
    )
    return jax.shard_map(
        on_device, mesh=mesh, in_specs=in_specs, out_specs=out_specs, check_vma=False
    )
```

```python
import functools

import jax
import jax.numpy as jnp
from jax import lax
from jax.experimental import pallas as pl
from jax.experimental.pallas import tpu as pltpu
from jax.sharding import PartitionSpec as P

D = 2048
HW = 1024
HEAD = 128


stat_decay = 0.9
moment_decay = 0.9
learn_rate = 0.02
highest = lax.Precision.HIGHEST
MESH = pl.DeviceIdType.MESH


def fold_one(carry_state, shard_piece, offset, root_mine, grad_mine):
    left_sum, outer_rows, column_total = carry_state
    row_count, col_width = shard_piece.shape
    left_sum = left_sum + jnp.dot(root_mine, shard_piece, precision=highest)
    outer_piece = lax.dot_general(
        grad_mine, shard_piece, (((1,), (1,)), ((), ())), precision=highest
    )
    outer_rows = lax.dynamic_update_slice_in_dim(outer_rows, outer_piece, offset, 1)
    by_head = shard_piece.reshape(row_count, col_width // HEAD, HEAD)
    column_total = column_total + jnp.einsum("rhi,rhj->hij", by_head, by_head, precision=highest)
    return (left_sum, outer_rows, column_total)


def finish(weight, moment, rows, cols, col_root, left_sum, outer_rows, column_total, square):
    norm_scale = jnp.sqrt(D * HW / (square + 1.0))
    scale_twice = norm_scale * norm_scale
    rows_next = stat_decay * rows + (1.0 - stat_decay) / HW * scale_twice * outer_rows
    cols_next = stat_decay * cols + (1.0 - stat_decay) / D * scale_twice * column_total
    shard_rows, col_width = left_sum.shape
    shaped = left_sum.reshape(shard_rows, col_width // HEAD, HEAD)
    precond = norm_scale * jnp.einsum(
        "rhi,hij->rhj", shaped, col_root.astype(jnp.float32), precision=highest
    ).reshape(shard_rows, col_width)
    moment_next = moment_decay * moment + (1.0 - moment_decay) * precond
    update_step = moment_decay * moment_next + (1.0 - moment_decay) * precond
    master = weight - learn_rate * update_step
    return (master, master.astype(jnp.bfloat16), update_step, moment_next, rows_next, cols_next)


def reduce_plan(
    inputs,
    query_grad,
    forget_grad,
    forget_pre,
    lower_bound,
    query_weight,
    forget_weight,
    query_moment,
    forget_moment,
    query_rows,
    forget_rows,
    query_cols,
    forget_cols,
    query_row_root,
    forget_row_root,
    query_col_root,
    forget_col_root,
):
    sigma_gate = jax.nn.sigmoid(forget_pre.astype(jnp.float32))
    forget_cot = (
        forget_grad.astype(jnp.float32) * (1.0 - lower_bound) * sigma_gate * (1.0 - sigma_gate)
    ).astype(jnp.bfloat16)
    gathered = lax.all_gather(inputs, "tp", axis=1, tiled=True)
    shard_rows, col_width = query_weight.shape
    heads_here = col_width // HEAD
    row_roots = (query_row_root.astype(jnp.float32), forget_row_root.astype(jnp.float32))
    empty = (
        jnp.zeros((shard_rows, col_width), jnp.float32),
        jnp.zeros((shard_rows, D), jnp.float32),
        jnp.zeros((heads_here, HEAD, HEAD), jnp.float32),
    )
    joined = jnp.concatenate([query_grad, forget_cot], axis=1)
    summed = lax.psum_scatter(
        lax.dot_general(
            gathered, joined, (((0,), (0,)), ((), ())), preferred_element_type=jnp.float32
        ),
        "fs",
        scatter_dimension=0,
        tiled=True,
    )
    gradients = (summed[:, :col_width], summed[:, col_width:])
    offset = jnp.int32(0)
    results = (
        fold_one(
            empty,
            lax.all_gather(gradients[0].astype(jnp.bfloat16), "fs", axis=0, tiled=True).astype(
                jnp.float32
            ),
            offset,
            row_roots[0],
            gradients[0],
        ),
        fold_one(
            empty,
            lax.all_gather(gradients[1].astype(jnp.bfloat16), "fs", axis=0, tiled=True).astype(
                jnp.float32
            ),
            offset,
            row_roots[1],
            gradients[1],
        ),
    )
    query_trace = jnp.sum(jnp.diagonal(results[0][2], axis1=1, axis2=2))
    forget_trace = jnp.sum(jnp.diagonal(results[1][2], axis1=1, axis2=2))
    query_outer, forget_outer, query_square, forget_square = (
        lax.psum(results[0][1].astype(jnp.bfloat16), "tp").astype(jnp.float32),
        lax.psum(results[1][1].astype(jnp.bfloat16), "tp").astype(jnp.float32),
        lax.psum(query_trace.astype(jnp.bfloat16), "tp").astype(jnp.float32),
        lax.psum(forget_trace.astype(jnp.bfloat16), "tp").astype(jnp.float32),
    )
    query_out = finish(
        query_weight,
        query_moment,
        query_rows,
        query_cols,
        query_col_root,
        results[0][0],
        query_outer,
        results[0][2],
        query_square,
    )
    forget_out = finish(
        forget_weight,
        forget_moment,
        forget_rows,
        forget_cols,
        forget_col_root,
        results[1][0],
        forget_outer,
        results[1][2],
        forget_square,
    )
    return (
        query_out[0],
        forget_out[0],
        query_out[1],
        forget_out[1],
        query_out[2],
        forget_out[2],
        query_out[3],
        forget_out[3],
        query_out[4],
        forget_out[4],
        query_out[5],
        forget_out[5],
    )


def to_bf16(value):
    return value.astype(jnp.bfloat16)


def wide_dot(left, right, dims):
    return lax.dot_general(left, right, (dims, ((), ())), preferred_element_type=jnp.float32)


def relay_kernel(
    x_ref, g_ref, rq_ref, rf_ref, cq_ref, cf_ref,
    s_ref, pq_ref, pf_ref, kq_ref, kf_ref,
    xs, gs, xt, acc, other, grad, owned, left, norms, own_sem, send_sem, recv_sem, swap_sem,
):
    shards = xs.shape[0]
    depth = shards // 2
    block, span = x_ref.shape
    fs = lax.axis_index("fs")
    tp = lax.axis_index("tp")
    z, px = lax.div(fs, 2), lax.rem(fs, 2)
    py, pc = lax.div(tp, 2), lax.rem(tp, 2)
    fs_other = fs + 1 - 2 * px
    tp_other = tp + 2 - 4 * py
    beside = {
        "up": (fs + 2, tp),
        "down": (fs - 2, tp),
        "x": (fs_other, tp),
        "y": (fs, tp_other),
        "core": (fs, tp + 1 - 2 * pc),
    }
    has_up = z < depth - 1
    has_down = z > 0

    def guarded(cond, action):
        if cond is None:
            action()
        else:
            pl.when(cond)(action)

    barrier = pltpu.get_barrier_semaphore()

    def greet(name):
        pl.semaphore_signal(barrier, inc=1, device_id=beside[name], device_id_type=MESH)

    for name in ("x", "y", "core"):
        greet(name)
    guarded(has_up, lambda: greet("up"))
    guarded(has_down, lambda: greet("down"))
    pl.semaphore_wait(
        barrier, 3 + jnp.where(has_up, 1, 0) + jnp.where(has_down, 1, 0)
    )

    slots = (xs, gs)
    pending = []

    def place(kind, slot, half):
        if kind == 1 and half is not None:
            return slots[kind].at[slot[0], slot[1], half]
        return slots[kind].at[slot[0], slot[1]]

    def copy_of(kind, src, slot, name, number, half=None):
        return pltpu.make_async_remote_copy(
            src_ref=src,
            dst_ref=place(kind, slot, half),
            send_sem=send_sem.at[number],
            recv_sem=recv_sem.at[kind, slot[0], slot[1]],
            device_id=beside[name],
            device_id_type=MESH,
        )

    def send(kind, src, slot, name, cond=None):
        number = len(pending)
        half = 1 - pc if name == "core" else None
        if kind == 1 and half is not None:
            src = src.at[half]
        build = functools.partial(copy_of, kind, src, slot, name, number, half)
        guarded(cond, lambda: build().start())
        pending.append((cond, build))

    def arrive(kind, slot, cond=None, half=None):
        here = place(kind, slot, half)
        guarded(cond, lambda: copy_of(kind, here, slot, "core", 0, half).wait_recv())

    def forward(kind, slot, names, cond=None):
        for name in names:
            send(kind, slots[kind].at[slot[0], slot[1]], slot, name, cond)

    own = (fs, tp)
    orders = (("x", "y"), ("y", "x"))
    sources = (x_ref, g_ref)

    def crossed(kind, layer):
        if kind == 0:
            return (2 * layer + 1 - px, tp)
        return (2 * layer + px, tp_other)

    def lasts(kind, layer):
        if kind == 0:
            return ((2 * layer + px, tp_other), (2 * layer + 1 - px, tp_other))
        return ((2 * layer + 1 - px, tp), (2 * layer + 1 - px, tp_other))

    keep = [
        pltpu.make_async_copy(sources[kind], slots[kind].at[fs, tp], own_sem.at[kind])
        for kind in range(2)
    ]
    for kind in range(2):
        send(kind, sources[kind], own, "up", has_up)
        send(kind, sources[kind], own, "down", has_down)
    for kind in range(2):
        send(kind, sources[kind], own, orders[kind][0])
    for kind in range(2):
        send(kind, sources[kind], own, orders[kind][1])
        send(kind, sources[kind], own, "core")
        keep[kind].start()

    def finals(stage):
        for layer, cond in stage:
            for kind in range(2):
                for slot in lasts(kind, layer):
                    arrive(kind, slot, cond)
                    forward(kind, slot, ("core",), cond)

    width = gs.shape[4]
    parts = gs.shape[1]
    chunk = s_ref.shape[1]
    steps = acc.shape[0] // chunk
    own_lanes = pl.ds(pl.multiple_of(tp * width, width), width)
    low = jnp.minimum(z, depth - 1 - z)

    def layer_of(turn):
        if turn == 0:
            return z
        near = z - (turn + 1) // 2 if turn % 2 == 1 else z + turn // 2
        far = jnp.where(2 * z < depth, turn, depth - 1 - turn)
        return jnp.where(turn <= 2 * low, near, far)

    def multiply(turn):
        layer = layer_of(turn)
        for across in range(2):
            for part in range(2):
                slot = (2 * layer + across, 2 * part + 1 - pc)
                for kind in range(2):
                    arrive(kind, slot, half=pc)
        for across in range(2):
            for part in range(parts):
                block_t = xs[2 * layer + across, part].T
                xt[part * span : (part + 1) * span, across * block : (across + 1) * block] = block_t
        first, final = turn == 0, turn == depth - 1
        both = pl.ds(2 * layer, 2)

        def step_body(step, total):
            rows = pl.ds(pl.multiple_of(step * chunk, chunk), chunk)
            for part in range(parts):
                cot = gs[both, part, pc].reshape(2 * block, width)
                piece = wide_dot(xt[rows, :], cot, ((1,), (0,)))
                lanes = slice(part * width, (part + 1) * width)
                if not first:
                    piece = piece + acc[rows, lanes]
                if final:
                    grad[rows, lanes] = to_bf16(piece)
                    total = total + jnp.sum(piece * piece, axis=0, keepdims=True)
                else:
                    acc[rows, lanes] = piece
            cot = gs[both, tp, 1 - pc].reshape(2 * block, width)
            piece = wide_dot(xt[rows, :], cot, ((1,), (0,)))
            if not first:
                piece = piece + other[rows, :]
            if final:
                owned[1 - pc, rows, :] = to_bf16(piece)
            else:
                other[rows, :] = piece
            return total

        return lax.fori_loop(0, steps, step_body, jnp.zeros((1, width), jnp.float32))

    previous = None
    for distance in range(depth):
        stage = []
        if distance == 0:
            stage.append((z, None))
        else:
            stage.append((z - distance, z >= distance))
            stage.append((z + distance, z + distance < depth))
            for sign, (layer, cond) in zip((-1, 1), stage):
                for kind in range(2):
                    slot = (2 * layer + px, tp)
                    arrive(kind, slot, cond)
                    if sign < 0:
                        onward, onto = "up", jnp.logical_and(cond, has_up)
                    else:
                        onward, onto = "down", jnp.logical_and(cond, has_down)
                    if distance < depth - 1:
                        forward(kind, slot, (onward,), onto)
                    forward(kind, slot, orders[kind] + ("core",), cond)
        for layer, cond in stage:
            for kind in range(2):
                slot = crossed(kind, layer)
                arrive(kind, slot, cond)
                forward(kind, slot, (orders[kind][1], "core"), cond)
        if previous is not None:
            finals(previous)
            if distance == 1:
                for kind in range(2):
                    keep[kind].wait()
            multiply(distance - 1)
        previous = stage
    finals(previous)
    total = multiply(depth - 1)

    tp_core = (fs, tp + 1 - 2 * pc)
    square = jnp.sum(total, axis=1, keepdims=True)
    norms[0] = jnp.broadcast_to(square, norms.shape[1:])
    swap_norm = pltpu.make_async_remote_copy(
        src_ref=norms.at[0], dst_ref=norms.at[1],
        send_sem=swap_sem.at[0], recv_sem=swap_sem.at[1],
        device_id=tp_core, device_id_type=MESH,
    )
    swap_rows = pltpu.make_async_remote_copy(
        src_ref=s_ref.at[pc], dst_ref=s_ref.at[pc],
        send_sem=swap_sem.at[2], recv_sem=swap_sem.at[3],
        device_id=tp_core, device_id_type=MESH,
    )
    take_rows = pltpu.make_async_remote_copy(
        src_ref=s_ref.at[1 - pc], dst_ref=s_ref.at[1 - pc],
        send_sem=swap_sem.at[2], recv_sem=swap_sem.at[3],
        device_id=tp_core, device_id_type=MESH,
    )
    size = float(grad.shape[0] * grad.shape[1])
    outer_scale = (1.0 - stat_decay) / grad.shape[1] * (size / (square + 1.0))
    mine = pl.ds(pl.multiple_of(fs * chunk, chunk), chunk)

    @pl.loop(0, steps)
    def _(step):
        rows = pl.ds(pl.multiple_of(step * chunk, chunk), chunk)
        outer = wide_dot(grad[mine, :], grad[rows, :], ((1,), (1,)))
        s_ref[pc, :, rows] = to_bf16(outer * outer_scale)
        owned[pc, rows, :] = grad[rows, own_lanes]

    swap_norm.start()
    heads = width // HEAD
    left[...] = jnp.zeros_like(left)
    kq_ref[...] = jnp.zeros_like(kq_ref)
    kf_ref[...] = jnp.zeros_like(kf_ref)
    swap_rows.start()

    @pl.loop(0, steps)
    def _(step):
        rows = pl.ds(pl.multiple_of(step * chunk, chunk), chunk)
        for which, (root, col_ref) in enumerate(((rq_ref, kq_ref), (rf_ref, kf_ref))):
            part = owned[which, rows, :]
            left[which] += wide_dot(root[:, rows], part, ((1,), (0,)))
            for head in range(heads):
                piece = part[:, head * HEAD : (head + 1) * HEAD]
                col_ref[head] += wide_dot(piece, piece, ((0,), (0,)))

    swap_norm.wait()
    mine_sum, their_sum = norms[0, 0:1, 0:1], norms[1, 0:1, 0:1]
    sums = (
        jnp.where(pc == 0, mine_sum, their_sum),
        jnp.where(pc == 0, their_sum, mine_sum),
    )
    for which, (col_root, pre_ref, col_ref) in enumerate(
        ((cq_ref, pq_ref, kq_ref), (cf_ref, pf_ref, kf_ref))
    ):
        scale_twice = size / (sums[which] + 1.0)
        norm_scale = jnp.sqrt(scale_twice)
        for head in range(heads):
            lanes = slice(head * HEAD, (head + 1) * HEAD)
            col_ref[head] = col_ref[head] * ((1.0 - stat_decay) / grad.shape[0] * scale_twice)
            pre_ref[:, lanes] = norm_scale * wide_dot(
                to_bf16(left[which, :, lanes]), col_root[head], ((1,), (0,))
            )
    swap_rows.wait_send()
    take_rows.wait_recv()

    for cond, build in pending:
        guarded(cond, lambda build=build: build().wait_send())


def relayed_products(x, cots, query_root, forget_root, query_col_root, forget_col_root):
    shards, parts = lax.axis_size("fs"), lax.axis_size("tp")
    block, span = x.shape
    width = cots.shape[2]
    chunk, features = query_root.shape
    depth = shards // 2
    sends = 2 * (5 + 8 * (depth - 1) + 2 * (2 * depth - 1) + 2 * (2 * depth - 1))
    f32 = jnp.float32
    heads = query_col_root.shape
    vmem = pl.BlockSpec(memory_space=pltpu.VMEM)
    return pl.pallas_call(
        relay_kernel,
        out_shape=[
            jax.ShapeDtypeStruct((2, chunk, features), jnp.bfloat16),
            jax.ShapeDtypeStruct((chunk, width), f32),
            jax.ShapeDtypeStruct((chunk, width), f32),
            jax.ShapeDtypeStruct(heads, f32),
            jax.ShapeDtypeStruct(heads, f32),
        ],
        in_specs=[vmem] * 6,
        out_specs=[vmem] * 5,
        scratch_shapes=[
            pltpu.VMEM((shards, parts, block, span), jnp.bfloat16),
            pltpu.VMEM((shards, parts, 2, block, width), jnp.bfloat16),
            pltpu.VMEM((features, 2 * block), jnp.bfloat16),
            pltpu.VMEM((features, parts * width), f32),
            pltpu.VMEM((features, width), f32),
            pltpu.VMEM((features, parts * width), jnp.bfloat16),
            pltpu.VMEM((2, features, width), jnp.bfloat16),
            pltpu.VMEM((2, chunk, width), f32),
            pltpu.VMEM((2, 8, 128), f32),
            pltpu.SemaphoreType.DMA((2,)),
            pltpu.SemaphoreType.DMA((sends,)),
            pltpu.SemaphoreType.DMA((2, shards, parts)),
            pltpu.SemaphoreType.DMA((4,)),
        ],
        compiler_params=pltpu.CompilerParams(
            collective_id=0, has_side_effects=True, vmem_limit_bytes=30 * 1024 * 1024
        ),
    )(x, cots, query_root, forget_root, query_col_root, forget_col_root)


def pack_kernel(query_ref, forget_ref, pre_ref, bound_ref, out_ref):
    out_ref[0] = query_ref[...]
    sigma_gate = jax.nn.sigmoid(pre_ref[...].astype(jnp.float32))
    out_ref[1] = to_bf16(
        forget_ref[...].astype(jnp.float32)
        * (1.0 - bound_ref[...])
        * sigma_gate
        * (1.0 - sigma_gate)
    )


def packed_cotangents(query_grad, forget_grad, forget_pre, lower_bound):
    vmem = pl.BlockSpec(memory_space=pltpu.VMEM)
    return pl.pallas_call(
        pack_kernel,
        out_shape=jax.ShapeDtypeStruct((2,) + query_grad.shape, jnp.bfloat16),
        in_specs=[vmem] * 4,
        out_specs=vmem,
        compiler_params=pltpu.CompilerParams(vmem_limit_bytes=4 * 1024 * 1024),
    )(query_grad, forget_grad, forget_pre, lower_bound.reshape(1, -1))


def finish_update(weight, moment, rows, cols, outer, precond, column):
    rows_next = stat_decay * rows + outer.astype(jnp.float32)
    cols_next = stat_decay * cols + column
    moment_next = moment_decay * moment + (1.0 - moment_decay) * precond
    update_step = moment_decay * moment_next + (1.0 - moment_decay) * precond
    master = weight - learn_rate * update_step
    return (master, to_bf16(master), update_step, moment_next, rows_next, cols_next)


def gather_plan(
    inputs,
    query_grad,
    forget_grad,
    forget_pre,
    lower_bound,
    query_weight,
    forget_weight,
    query_moment,
    forget_moment,
    query_rows,
    forget_rows,
    query_cols,
    forget_cols,
    query_row_root,
    forget_row_root,
    query_col_root,
    forget_col_root,
):
    outers, query_pre, forget_pre_out, query_column, forget_column = relayed_products(
        inputs,
        packed_cotangents(query_grad, forget_grad, forget_pre, lower_bound),
        query_row_root,
        forget_row_root,
        query_col_root,
        forget_col_root,
    )
    query_outer, forget_outer = outers[0], outers[1]
    query_out = finish_update(
        query_weight, query_moment, query_rows, query_cols, query_outer, query_pre, query_column
    )
    forget_out = finish_update(
        forget_weight, forget_moment, forget_rows, forget_cols,
        forget_outer, forget_pre_out, forget_column,
    )
    return tuple(piece for pair in zip(query_out, forget_out) for piece in pair)


def on_device(*args):
    token_count = args[0].shape[0] * lax.axis_size("fs")
    feature_count = args[0].shape[1] * lax.axis_size("tp")
    paired = lax.axis_size("fs") % 2 == 0 and lax.axis_size("tp") == 4
    if paired and token_count <= feature_count:
        return gather_plan(*args)
    return reduce_plan(*args)


def solution(mesh):
    in_specs = (
        P("fs", "tp"),
        P("fs", "tp"),
        P("fs", "tp"),
        P("fs", "tp"),
        P("tp"),
        P("fs", "tp"),
        P("fs", "tp"),
        P("fs", "tp"),
        P("fs", "tp"),
        P("fs", None),
        P("fs", None),
        P("tp", None, None),
        P("tp", None, None),
        P("fs", None),
        P("fs", None),
        P("tp", None, None),
        P("tp", None, None),
    )
    out_specs = (
        P("fs", "tp"),
        P("fs", "tp"),
        P("fs", "tp"),
        P("fs", "tp"),
        P("fs", "tp"),
        P("fs", "tp"),
        P("fs", "tp"),
        P("fs", "tp"),
        P("fs", None),
        P("fs", None),
        P("tp", None, None),
        P("tp", None, None),
    )
    return jax.shard_map(
        on_device, mesh=mesh, in_specs=in_specs, out_specs=out_specs, check_vma=False
    )
```

```python
import functools

import jax
import jax.numpy as jnp
from jax import lax
from jax.experimental import pallas as pl
from jax.experimental.pallas import tpu as pltpu
from jax.sharding import PartitionSpec as P

D = 2048
HW = 1024
HEAD = 128


stat_decay = 0.9
moment_decay = 0.9
learn_rate = 0.02
highest = lax.Precision.HIGHEST
MESH = pl.DeviceIdType.MESH


def fold_one(carry_state, shard_piece, offset, root_mine, grad_mine):
    left_sum, outer_rows, column_total = carry_state
    row_count, col_width = shard_piece.shape
    left_sum = left_sum + jnp.dot(root_mine, shard_piece, precision=highest)
    outer_piece = lax.dot_general(
        grad_mine, shard_piece, (((1,), (1,)), ((), ())), precision=highest
    )
    outer_rows = lax.dynamic_update_slice_in_dim(outer_rows, outer_piece, offset, 1)
    by_head = shard_piece.reshape(row_count, col_width // HEAD, HEAD)
    column_total = column_total + jnp.einsum("rhi,rhj->hij", by_head, by_head, precision=highest)
    return (left_sum, outer_rows, column_total)


def finish(weight, moment, rows, cols, col_root, left_sum, outer_rows, column_total, square):
    norm_scale = jnp.sqrt(D * HW / (square + 1.0))
    scale_twice = norm_scale * norm_scale
    rows_next = stat_decay * rows + (1.0 - stat_decay) / HW * scale_twice * outer_rows
    cols_next = stat_decay * cols + (1.0 - stat_decay) / D * scale_twice * column_total
    shard_rows, col_width = left_sum.shape
    shaped = left_sum.reshape(shard_rows, col_width // HEAD, HEAD)
    precond = norm_scale * jnp.einsum(
        "rhi,hij->rhj", shaped, col_root.astype(jnp.float32), precision=highest
    ).reshape(shard_rows, col_width)
    moment_next = moment_decay * moment + (1.0 - moment_decay) * precond
    update_step = moment_decay * moment_next + (1.0 - moment_decay) * precond
    master = weight - learn_rate * update_step
    return (master, master.astype(jnp.bfloat16), update_step, moment_next, rows_next, cols_next)


def reduce_plan(
    inputs,
    query_grad,
    forget_grad,
    forget_pre,
    lower_bound,
    query_weight,
    forget_weight,
    query_moment,
    forget_moment,
    query_rows,
    forget_rows,
    query_cols,
    forget_cols,
    query_row_root,
    forget_row_root,
    query_col_root,
    forget_col_root,
):
    sigma_gate = jax.nn.sigmoid(forget_pre.astype(jnp.float32))
    forget_cot = (
        forget_grad.astype(jnp.float32) * (1.0 - lower_bound) * sigma_gate * (1.0 - sigma_gate)
    ).astype(jnp.bfloat16)
    gathered = lax.all_gather(inputs, "tp", axis=1, tiled=True)
    shard_rows, col_width = query_weight.shape
    heads_here = col_width // HEAD
    row_roots = (query_row_root.astype(jnp.float32), forget_row_root.astype(jnp.float32))
    empty = (
        jnp.zeros((shard_rows, col_width), jnp.float32),
        jnp.zeros((shard_rows, D), jnp.float32),
        jnp.zeros((heads_here, HEAD, HEAD), jnp.float32),
    )
    joined = jnp.concatenate([query_grad, forget_cot], axis=1)
    summed = lax.psum_scatter(
        lax.dot_general(
            gathered, joined, (((0,), (0,)), ((), ())), preferred_element_type=jnp.float32
        ),
        "fs",
        scatter_dimension=0,
        tiled=True,
    )
    gradients = (summed[:, :col_width], summed[:, col_width:])
    offset = jnp.int32(0)
    results = (
        fold_one(
            empty,
            lax.all_gather(gradients[0].astype(jnp.bfloat16), "fs", axis=0, tiled=True).astype(
                jnp.float32
            ),
            offset,
            row_roots[0],
            gradients[0],
        ),
        fold_one(
            empty,
            lax.all_gather(gradients[1].astype(jnp.bfloat16), "fs", axis=0, tiled=True).astype(
                jnp.float32
            ),
            offset,
            row_roots[1],
            gradients[1],
        ),
    )
    query_trace = jnp.sum(jnp.diagonal(results[0][2], axis1=1, axis2=2))
    forget_trace = jnp.sum(jnp.diagonal(results[1][2], axis1=1, axis2=2))
    query_outer, forget_outer, query_square, forget_square = (
        lax.psum(results[0][1].astype(jnp.bfloat16), "tp").astype(jnp.float32),
        lax.psum(results[1][1].astype(jnp.bfloat16), "tp").astype(jnp.float32),
        lax.psum(query_trace.astype(jnp.bfloat16), "tp").astype(jnp.float32),
        lax.psum(forget_trace.astype(jnp.bfloat16), "tp").astype(jnp.float32),
    )
    query_out = finish(
        query_weight,
        query_moment,
        query_rows,
        query_cols,
        query_col_root,
        results[0][0],
        query_outer,
        results[0][2],
        query_square,
    )
    forget_out = finish(
        forget_weight,
        forget_moment,
        forget_rows,
        forget_cols,
        forget_col_root,
        results[1][0],
        forget_outer,
        results[1][2],
        forget_square,
    )
    return (
        query_out[0],
        forget_out[0],
        query_out[1],
        forget_out[1],
        query_out[2],
        forget_out[2],
        query_out[3],
        forget_out[3],
        query_out[4],
        forget_out[4],
        query_out[5],
        forget_out[5],
    )


def to_bf16(value):
    return value.astype(jnp.bfloat16)


def wide_dot(left, right, dims):
    return lax.dot_general(left, right, (dims, ((), ())), preferred_element_type=jnp.float32)


def relay_kernel(
    x_ref, g_ref, rq_hbm, rf_hbm, cq_ref, cf_ref,
    s_ref, pq_ref, pf_ref, kq_ref, kf_ref,
    xs, gs, xt, acc, other, grad, owned, left, norms, roots, own_sem, send_sem, recv_sem, swap_sem,
):
    shards = xs.shape[0]
    depth = shards // 2
    block, span = x_ref.shape
    fs = lax.axis_index("fs")
    tp = lax.axis_index("tp")
    z, px = lax.div(fs, 2), lax.rem(fs, 2)
    py, pc = lax.div(tp, 2), lax.rem(tp, 2)
    fs_other = fs + 1 - 2 * px
    tp_other = tp + 2 - 4 * py
    beside = {
        "up": (fs + 2, tp),
        "down": (fs - 2, tp),
        "x": (fs_other, tp),
        "y": (fs, tp_other),
        "core": (fs, tp + 1 - 2 * pc),
    }
    has_up = z < depth - 1
    has_down = z > 0

    def guarded(cond, action):
        if cond is None:
            action()
        else:
            pl.when(cond)(action)

    barrier = pltpu.get_barrier_semaphore()

    def greet(name):
        pl.semaphore_signal(barrier, inc=1, device_id=beside[name], device_id_type=MESH)

    for name in ("x", "y", "core"):
        greet(name)
    guarded(has_up, lambda: greet("up"))
    guarded(has_down, lambda: greet("down"))
    pl.semaphore_wait(
        barrier, 3 + jnp.where(has_up, 1, 0) + jnp.where(has_down, 1, 0)
    )

    slots = (xs, gs)
    pending = []

    def place(kind, slot, half):
        if kind == 1 and half is not None:
            return slots[kind].at[slot[0], slot[1], half]
        return slots[kind].at[slot[0], slot[1]]

    def copy_of(kind, src, slot, name, number, half=None):
        return pltpu.make_async_remote_copy(
            src_ref=src,
            dst_ref=place(kind, slot, half),
            send_sem=send_sem.at[number],
            recv_sem=recv_sem.at[kind, slot[0], slot[1]],
            device_id=beside[name],
            device_id_type=MESH,
        )

    def send(kind, src, slot, name, cond=None):
        number = len(pending)
        half = 1 - pc if name == "core" else None
        if kind == 1 and half is not None:
            src = src.at[half]
        build = functools.partial(copy_of, kind, src, slot, name, number, half)
        guarded(cond, lambda: build().start())
        pending.append((cond, build))

    def arrive(kind, slot, cond=None, half=None):
        here = place(kind, slot, half)
        guarded(cond, lambda: copy_of(kind, here, slot, "core", 0, half).wait_recv())

    def forward(kind, slot, names, cond=None):
        for name in names:
            send(kind, slots[kind].at[slot[0], slot[1]], slot, name, cond)

    own = (fs, tp)
    orders = (("x", "y"), ("y", "x"))
    sources = (x_ref, g_ref)

    def crossed(kind, layer):
        if kind == 0:
            return (2 * layer + 1 - px, tp)
        return (2 * layer + px, tp_other)

    def lasts(kind, layer):
        if kind == 0:
            return ((2 * layer + px, tp_other), (2 * layer + 1 - px, tp_other))
        return ((2 * layer + 1 - px, tp), (2 * layer + 1 - px, tp_other))

    keep = [
        pltpu.make_async_copy(sources[kind], slots[kind].at[fs, tp], own_sem.at[kind])
        for kind in range(2)
    ]
    loads = [
        pltpu.make_async_copy(source, roots.at[which], own_sem.at[2 + which])
        for which, source in enumerate((rq_hbm, rf_hbm))
    ]
    for kind in range(2):
        send(kind, sources[kind], own, "up", has_up)
        send(kind, sources[kind], own, "down", has_down)
    for kind in range(2):
        send(kind, sources[kind], own, orders[kind][0])
    for kind in range(2):
        send(kind, sources[kind], own, orders[kind][1])
        send(kind, sources[kind], own, "core")
        keep[kind].start()
        loads[kind].start()

    def finals(stage):
        for layer, cond in stage:
            for kind in range(2):
                for slot in lasts(kind, layer):
                    arrive(kind, slot, cond)
                    forward(kind, slot, ("core",), cond)

    width = gs.shape[4]
    parts = gs.shape[1]
    chunk = s_ref.shape[1]
    steps = acc.shape[0] // chunk
    own_lanes = pl.ds(pl.multiple_of(tp * width, width), width)
    low = jnp.minimum(z, depth - 1 - z)

    def layer_of(turn):
        if turn == 0:
            return z
        near = z - (turn + 1) // 2 if turn % 2 == 1 else z + turn // 2
        far = jnp.where(2 * z < depth, turn, depth - 1 - turn)
        return jnp.where(turn <= 2 * low, near, far)

    def multiply(turn):
        layer = layer_of(turn)
        for across in range(2):
            for part in range(2):
                slot = (2 * layer + across, 2 * part + 1 - pc)
                for kind in range(2):
                    arrive(kind, slot, half=pc)
        for across in range(2):
            for part in range(parts):
                block_t = xs[2 * layer + across, part].T
                xt[part * span : (part + 1) * span, across * block : (across + 1) * block] = block_t
        first, final = turn == 0, turn == depth - 1
        both = pl.ds(2 * layer, 2)

        def step_body(step, total):
            rows = pl.ds(pl.multiple_of(step * chunk, chunk), chunk)
            for part in range(parts):
                cot = gs[both, part, pc].reshape(2 * block, width)
                piece = wide_dot(xt[rows, :], cot, ((1,), (0,)))
                lanes = slice(part * width, (part + 1) * width)
                if not first:
                    piece = piece + acc[rows, lanes]
                if final:
                    grad[rows, lanes] = to_bf16(piece)
                    total = total + jnp.sum(piece * piece, axis=0, keepdims=True)
                else:
                    acc[rows, lanes] = piece
            cot = gs[both, tp, 1 - pc].reshape(2 * block, width)
            piece = wide_dot(xt[rows, :], cot, ((1,), (0,)))
            if not first:
                piece = piece + other[rows, :]
            if final:
                owned[1 - pc, rows, :] = to_bf16(piece)
            else:
                other[rows, :] = piece
            return total

        return lax.fori_loop(0, steps, step_body, jnp.zeros((1, width), jnp.float32))

    def layers_at(distance):
        if distance == 0:
            return ((z, None),)
        return (
            (z - distance, z >= distance),
            (z + distance, z + distance < depth),
        )

    def along(distance):
        for onward, (layer, cond), more in zip(
            ("up", "down"), layers_at(distance), (has_up, has_down)
        ):
            for kind in range(2):
                slot = (2 * layer + px, tp)
                arrive(kind, slot, cond)
                if distance < depth - 1:
                    forward(kind, slot, (onward,), jnp.logical_and(cond, more))
                forward(kind, slot, orders[kind] + ("core",), cond)

    def across_pair(distance):
        for layer, cond in layers_at(distance):
            for kind in range(2):
                slot = crossed(kind, layer)
                arrive(kind, slot, cond)
                forward(kind, slot, (orders[kind][1], "core"), cond)

    for distance in range(1, depth):
        along(distance)
        across_pair(distance - 1)
    finals(layers_at(0))
    for kind in range(2):
        keep[kind].wait()
    multiply(0)
    across_pair(depth - 1)
    for distance in range(1, depth - 1):
        finals(layers_at(distance))
        multiply(distance)
    finals(layers_at(depth - 1))
    total = multiply(depth - 1)

    tp_core = (fs, tp + 1 - 2 * pc)
    square = jnp.sum(total, axis=1, keepdims=True)
    norms[0] = jnp.broadcast_to(square, norms.shape[1:])
    swap_norm = pltpu.make_async_remote_copy(
        src_ref=norms.at[0], dst_ref=norms.at[1],
        send_sem=swap_sem.at[0], recv_sem=swap_sem.at[1],
        device_id=tp_core, device_id_type=MESH,
    )
    swap_rows = pltpu.make_async_remote_copy(
        src_ref=s_ref.at[pc], dst_ref=s_ref.at[pc],
        send_sem=swap_sem.at[2], recv_sem=swap_sem.at[3],
        device_id=tp_core, device_id_type=MESH,
    )
    take_rows = pltpu.make_async_remote_copy(
        src_ref=s_ref.at[1 - pc], dst_ref=s_ref.at[1 - pc],
        send_sem=swap_sem.at[2], recv_sem=swap_sem.at[3],
        device_id=tp_core, device_id_type=MESH,
    )
    size = float(grad.shape[0] * grad.shape[1])
    outer_scale = (1.0 - stat_decay) / grad.shape[1] * (size / (square + 1.0))
    mine = pl.ds(pl.multiple_of(fs * chunk, chunk), chunk)

    @pl.loop(0, steps)
    def _(step):
        rows = pl.ds(pl.multiple_of(step * chunk, chunk), chunk)
        outer = wide_dot(grad[mine, :], grad[rows, :], ((1,), (1,)))
        s_ref[pc, :, rows] = to_bf16(outer * outer_scale)
        owned[pc, rows, :] = grad[rows, own_lanes]

    swap_norm.start()
    heads = width // HEAD
    left[...] = jnp.zeros_like(left)
    kq_ref[...] = jnp.zeros_like(kq_ref)
    kf_ref[...] = jnp.zeros_like(kf_ref)
    swap_rows.start()
    for load in loads:
        load.wait()

    @pl.loop(0, steps)
    def _(step):
        rows = pl.ds(pl.multiple_of(step * chunk, chunk), chunk)
        for which, (root, col_ref) in enumerate(((roots.at[0], kq_ref), (roots.at[1], kf_ref))):
            part = owned[which, rows, :]
            left[which] += wide_dot(root[:, rows], part, ((1,), (0,)))
            for head in range(heads):
                piece = part[:, head * HEAD : (head + 1) * HEAD]
                col_ref[head] += wide_dot(piece, piece, ((0,), (0,)))

    swap_norm.wait()
    mine_sum, their_sum = norms[0, 0:1, 0:1], norms[1, 0:1, 0:1]
    sums = (
        jnp.where(pc == 0, mine_sum, their_sum),
        jnp.where(pc == 0, their_sum, mine_sum),
    )
    for which, (col_root, pre_ref, col_ref) in enumerate(
        ((cq_ref, pq_ref, kq_ref), (cf_ref, pf_ref, kf_ref))
    ):
        scale_twice = size / (sums[which] + 1.0)
        norm_scale = jnp.sqrt(scale_twice)
        for head in range(heads):
            lanes = slice(head * HEAD, (head + 1) * HEAD)
            col_ref[head] = col_ref[head] * ((1.0 - stat_decay) / grad.shape[0] * scale_twice)
            pre_ref[:, lanes] = norm_scale * wide_dot(
                to_bf16(left[which, :, lanes]), col_root[head], ((1,), (0,))
            )
    swap_rows.wait_send()
    take_rows.wait_recv()

    for cond, build in pending:
        guarded(cond, lambda build=build: build().wait_send())


def relayed_products(x, cots, query_root, forget_root, query_col_root, forget_col_root):
    shards, parts = lax.axis_size("fs"), lax.axis_size("tp")
    block, span = x.shape
    width = cots.shape[2]
    chunk, features = query_root.shape
    depth = shards // 2
    sends = 2 * (5 + 8 * (depth - 1) + 2 * (2 * depth - 1) + 2 * (2 * depth - 1))
    f32 = jnp.float32
    heads = query_col_root.shape
    vmem = pl.BlockSpec(memory_space=pltpu.VMEM)
    hbm = pl.BlockSpec(memory_space=pltpu.HBM)
    return pl.pallas_call(
        relay_kernel,
        out_shape=[
            jax.ShapeDtypeStruct((2, chunk, features), jnp.bfloat16),
            jax.ShapeDtypeStruct((chunk, width), f32),
            jax.ShapeDtypeStruct((chunk, width), f32),
            jax.ShapeDtypeStruct(heads, f32),
            jax.ShapeDtypeStruct(heads, f32),
        ],
        in_specs=[vmem, vmem, hbm, hbm, vmem, vmem],
        out_specs=[vmem] * 5,
        scratch_shapes=[
            pltpu.VMEM((shards, parts, block, span), jnp.bfloat16),
            pltpu.VMEM((shards, parts, 2, block, width), jnp.bfloat16),
            pltpu.VMEM((features, 2 * block), jnp.bfloat16),
            pltpu.VMEM((features, parts * width), f32),
            pltpu.VMEM((features, width), f32),
            pltpu.VMEM((features, parts * width), jnp.bfloat16),
            pltpu.VMEM((2, features, width), jnp.bfloat16),
            pltpu.VMEM((2, chunk, width), f32),
            pltpu.VMEM((2, 8, 128), f32),
            pltpu.VMEM((2, chunk, features), jnp.bfloat16),
            pltpu.SemaphoreType.DMA((4,)),
            pltpu.SemaphoreType.DMA((sends,)),
            pltpu.SemaphoreType.DMA((2, shards, parts)),
            pltpu.SemaphoreType.DMA((4,)),
        ],
        compiler_params=pltpu.CompilerParams(
            collective_id=0, has_side_effects=True, vmem_limit_bytes=61 * 1024 * 1024
        ),
    )(x, cots, query_root, forget_root, query_col_root, forget_col_root)


def pack_kernel(query_ref, forget_ref, pre_ref, bound_ref, out_ref):
    out_ref[0] = query_ref[...]
    sigma_gate = jax.nn.sigmoid(pre_ref[...].astype(jnp.float32))
    out_ref[1] = to_bf16(
        forget_ref[...].astype(jnp.float32)
        * (1.0 - bound_ref[...])
        * sigma_gate
        * (1.0 - sigma_gate)
    )


def packed_cotangents(query_grad, forget_grad, forget_pre, lower_bound):
    vmem = pl.BlockSpec(memory_space=pltpu.VMEM)
    return pl.pallas_call(
        pack_kernel,
        out_shape=jax.ShapeDtypeStruct((2,) + query_grad.shape, jnp.bfloat16),
        in_specs=[vmem] * 4,
        out_specs=vmem,
        compiler_params=pltpu.CompilerParams(vmem_limit_bytes=61 * 1024 * 1024),
    )(query_grad, forget_grad, forget_pre, lower_bound.reshape(1, -1))


def finish_kernel(outer_ref, *refs):
    pres, columns, weights, moments, rows, cols = (refs[2 * k : 2 * k + 2] for k in range(6))
    outs = refs[12:]
    for which in range(2):
        master_ref, copy_ref, step_ref, moment_ref, rows_ref, cols_ref = outs[which::2]
        precond = pres[which][...]
        moment_next = moment_decay * moments[which][...] + (1.0 - moment_decay) * precond
        update_step = moment_decay * moment_next + (1.0 - moment_decay) * precond
        master = weights[which][...] - learn_rate * update_step
        master_ref[...] = master
        copy_ref[...] = to_bf16(master)
        step_ref[...] = update_step
        moment_ref[...] = moment_next
        rows_ref[...] = stat_decay * rows[which][...] + outer_ref[which].astype(jnp.float32)
        cols_ref[...] = stat_decay * cols[which][...] + columns[which][...]


def finished(outers, pres, columns, weights, moments, rows, cols):
    f32, bf16 = jnp.float32, jnp.bfloat16
    chunk, width = weights[0].shape
    features = rows[0].shape[1]
    heads = cols[0].shape
    steps = 4
    tile = chunk // steps
    narrow = pl.BlockSpec((tile, width), lambda i: (i, 0))
    wide = pl.BlockSpec((tile, features), lambda i: (i, 0))
    head = pl.BlockSpec((heads[0], heads[1] // steps, heads[2]), lambda i: (0, i, 0))
    both = pl.BlockSpec((2, tile, features), lambda i: (0, i, 0))
    flat = lambda kind: [jax.ShapeDtypeStruct((chunk, width), kind)] * 2
    return pl.pallas_call(
        finish_kernel,
        grid=(steps,),
        out_shape=flat(f32)
        + flat(bf16)
        + flat(f32)
        + flat(f32)
        + [jax.ShapeDtypeStruct((chunk, features), f32)] * 2
        + [jax.ShapeDtypeStruct(heads, f32)] * 2,
        in_specs=[both] + [narrow] * 2 + [head] * 2 + [narrow] * 4 + [wide] * 2 + [head] * 2,
        out_specs=[narrow] * 8 + [wide] * 2 + [head] * 2,
        compiler_params=pltpu.CompilerParams(vmem_limit_bytes=61 * 1024 * 1024),
    )(outers, *pres, *columns, *weights, *moments, *rows, *cols)


def gather_plan(
    inputs,
    query_grad,
    forget_grad,
    forget_pre,
    lower_bound,
    query_weight,
    forget_weight,
    query_moment,
    forget_moment,
    query_rows,
    forget_rows,
    query_cols,
    forget_cols,
    query_row_root,
    forget_row_root,
    query_col_root,
    forget_col_root,
):
    outers, query_pre, forget_pre_out, query_column, forget_column = relayed_products(
        inputs,
        packed_cotangents(query_grad, forget_grad, forget_pre, lower_bound),
        query_row_root,
        forget_row_root,
        query_col_root,
        forget_col_root,
    )
    return tuple(
        finished(
            outers,
            (query_pre, forget_pre_out),
            (query_column, forget_column),
            (query_weight, forget_weight),
            (query_moment, forget_moment),
            (query_rows, forget_rows),
            (query_cols, forget_cols),
        )
    )


def on_device(*args):
    token_count = args[0].shape[0] * lax.axis_size("fs")
    feature_count = args[0].shape[1] * lax.axis_size("tp")
    paired = lax.axis_size("fs") % 2 == 0 and lax.axis_size("tp") == 4
    if paired and token_count <= feature_count:
        return gather_plan(*args)
    return reduce_plan(*args)


def solution(mesh):
    in_specs = (
        P("fs", "tp"),
        P("fs", "tp"),
        P("fs", "tp"),
        P("fs", "tp"),
        P("tp"),
        P("fs", "tp"),
        P("fs", "tp"),
        P("fs", "tp"),
        P("fs", "tp"),
        P("fs", None),
        P("fs", None),
        P("tp", None, None),
        P("tp", None, None),
        P("fs", None),
        P("fs", None),
        P("tp", None, None),
        P("tp", None, None),
    )
    out_specs = (
        P("fs", "tp"),
        P("fs", "tp"),
        P("fs", "tp"),
        P("fs", "tp"),
        P("fs", "tp"),
        P("fs", "tp"),
        P("fs", "tp"),
        P("fs", "tp"),
        P("fs", None),
        P("fs", None),
        P("tp", None, None),
        P("tp", None, None),
    )
    return jax.shard_map(
        on_device, mesh=mesh, in_specs=in_specs, out_specs=out_specs, check_vma=False
    )
```

```python
import functools

import jax
import jax.numpy as jnp
from jax import lax
from jax.experimental import pallas as pl
from jax.experimental.pallas import tpu as pltpu
from jax.sharding import PartitionSpec as P

D = 2048
HW = 1024
HEAD = 128


stat_decay = 0.9
moment_decay = 0.9
learn_rate = 0.02
highest = lax.Precision.HIGHEST
MESH = pl.DeviceIdType.MESH


def fold_one(carry_state, shard_piece, offset, root_mine, grad_mine):
    left_sum, outer_rows, column_total = carry_state
    row_count, col_width = shard_piece.shape
    left_sum = left_sum + jnp.dot(root_mine, shard_piece, precision=highest)
    outer_piece = lax.dot_general(
        grad_mine, shard_piece, (((1,), (1,)), ((), ())), precision=highest
    )
    outer_rows = lax.dynamic_update_slice_in_dim(outer_rows, outer_piece, offset, 1)
    by_head = shard_piece.reshape(row_count, col_width // HEAD, HEAD)
    column_total = column_total + jnp.einsum("rhi,rhj->hij", by_head, by_head, precision=highest)
    return (left_sum, outer_rows, column_total)


def finish(weight, moment, rows, cols, col_root, left_sum, outer_rows, column_total, square):
    norm_scale = jnp.sqrt(D * HW / (square + 1.0))
    scale_twice = norm_scale * norm_scale
    rows_next = stat_decay * rows + (1.0 - stat_decay) / HW * scale_twice * outer_rows
    cols_next = stat_decay * cols + (1.0 - stat_decay) / D * scale_twice * column_total
    shard_rows, col_width = left_sum.shape
    shaped = left_sum.reshape(shard_rows, col_width // HEAD, HEAD)
    precond = norm_scale * jnp.einsum(
        "rhi,hij->rhj", shaped, col_root.astype(jnp.float32), precision=highest
    ).reshape(shard_rows, col_width)
    moment_next = moment_decay * moment + (1.0 - moment_decay) * precond
    update_step = moment_decay * moment_next + (1.0 - moment_decay) * precond
    master = weight - learn_rate * update_step
    return (master, master.astype(jnp.bfloat16), update_step, moment_next, rows_next, cols_next)


def reduce_plan(
    inputs,
    query_grad,
    forget_grad,
    forget_pre,
    lower_bound,
    query_weight,
    forget_weight,
    query_moment,
    forget_moment,
    query_rows,
    forget_rows,
    query_cols,
    forget_cols,
    query_row_root,
    forget_row_root,
    query_col_root,
    forget_col_root,
):
    sigma_gate = jax.nn.sigmoid(forget_pre.astype(jnp.float32))
    forget_cot = (
        forget_grad.astype(jnp.float32) * (1.0 - lower_bound) * sigma_gate * (1.0 - sigma_gate)
    ).astype(jnp.bfloat16)
    gathered = lax.all_gather(inputs, "tp", axis=1, tiled=True)
    shard_rows, col_width = query_weight.shape
    heads_here = col_width // HEAD
    row_roots = (query_row_root.astype(jnp.float32), forget_row_root.astype(jnp.float32))
    empty = (
        jnp.zeros((shard_rows, col_width), jnp.float32),
        jnp.zeros((shard_rows, D), jnp.float32),
        jnp.zeros((heads_here, HEAD, HEAD), jnp.float32),
    )
    joined = jnp.concatenate([query_grad, forget_cot], axis=1)
    summed = lax.psum_scatter(
        lax.dot_general(
            gathered, joined, (((0,), (0,)), ((), ())), preferred_element_type=jnp.float32
        ),
        "fs",
        scatter_dimension=0,
        tiled=True,
    )
    gradients = (summed[:, :col_width], summed[:, col_width:])
    offset = jnp.int32(0)
    results = (
        fold_one(
            empty,
            lax.all_gather(gradients[0].astype(jnp.bfloat16), "fs", axis=0, tiled=True).astype(
                jnp.float32
            ),
            offset,
            row_roots[0],
            gradients[0],
        ),
        fold_one(
            empty,
            lax.all_gather(gradients[1].astype(jnp.bfloat16), "fs", axis=0, tiled=True).astype(
                jnp.float32
            ),
            offset,
            row_roots[1],
            gradients[1],
        ),
    )
    query_trace = jnp.sum(jnp.diagonal(results[0][2], axis1=1, axis2=2))
    forget_trace = jnp.sum(jnp.diagonal(results[1][2], axis1=1, axis2=2))
    query_outer, forget_outer, query_square, forget_square = (
        lax.psum(results[0][1].astype(jnp.bfloat16), "tp").astype(jnp.float32),
        lax.psum(results[1][1].astype(jnp.bfloat16), "tp").astype(jnp.float32),
        lax.psum(query_trace.astype(jnp.bfloat16), "tp").astype(jnp.float32),
        lax.psum(forget_trace.astype(jnp.bfloat16), "tp").astype(jnp.float32),
    )
    query_out = finish(
        query_weight,
        query_moment,
        query_rows,
        query_cols,
        query_col_root,
        results[0][0],
        query_outer,
        results[0][2],
        query_square,
    )
    forget_out = finish(
        forget_weight,
        forget_moment,
        forget_rows,
        forget_cols,
        forget_col_root,
        results[1][0],
        forget_outer,
        results[1][2],
        forget_square,
    )
    return (
        query_out[0],
        forget_out[0],
        query_out[1],
        forget_out[1],
        query_out[2],
        forget_out[2],
        query_out[3],
        forget_out[3],
        query_out[4],
        forget_out[4],
        query_out[5],
        forget_out[5],
    )


def to_bf16(value):
    return value.astype(jnp.bfloat16)


def wide_dot(left, right, dims):
    return lax.dot_general(left, right, (dims, ((), ())), preferred_element_type=jnp.float32)


def relay_kernel(
    x_ref, g_ref, rq_hbm, rf_hbm, cq_ref, cf_ref,
    s_ref, pq_ref, pf_ref, kq_ref, kf_ref,
    xs, gs, xt, acc, other, grad, owned, left, norms, roots, own_sem, send_sem, recv_sem, swap_sem,
):
    shards = xs.shape[0]
    depth = shards // 2
    block, span = x_ref.shape
    fs = lax.axis_index("fs")
    tp = lax.axis_index("tp")
    z, px = lax.div(fs, 2), lax.rem(fs, 2)
    py, pc = lax.div(tp, 2), lax.rem(tp, 2)
    fs_other = fs + 1 - 2 * px
    tp_other = tp + 2 - 4 * py
    beside = {
        "up": (fs + 2, tp),
        "down": (fs - 2, tp),
        "x": (fs_other, tp),
        "y": (fs, tp_other),
        "core": (fs, tp + 1 - 2 * pc),
    }
    has_up = z < depth - 1
    has_down = z > 0

    def guarded(cond, action):
        if cond is None:
            action()
        else:
            pl.when(cond)(action)

    barrier = pltpu.get_barrier_semaphore()

    def greet(name):
        pl.semaphore_signal(barrier, inc=1, device_id=beside[name], device_id_type=MESH)

    for name in ("x", "y", "core"):
        greet(name)
    guarded(has_up, lambda: greet("up"))
    guarded(has_down, lambda: greet("down"))
    pl.semaphore_wait(
        barrier, 3 + jnp.where(has_up, 1, 0) + jnp.where(has_down, 1, 0)
    )

    slots = (xs, gs)
    pending = []

    def place(kind, slot, half):
        if kind == 1 and half is not None:
            return slots[kind].at[slot[0], slot[1], half]
        return slots[kind].at[slot[0], slot[1]]

    def copy_of(kind, src, slot, name, number, half=None):
        return pltpu.make_async_remote_copy(
            src_ref=src,
            dst_ref=place(kind, slot, half),
            send_sem=send_sem.at[number],
            recv_sem=recv_sem.at[kind, slot[0], slot[1]],
            device_id=beside[name],
            device_id_type=MESH,
        )

    def send(kind, src, slot, name, cond=None):
        number = len(pending)
        half = 1 - pc if name == "core" else None
        if kind == 1 and half is not None:
            src = src.at[half]
        build = functools.partial(copy_of, kind, src, slot, name, number, half)
        guarded(cond, lambda: build().start())
        pending.append((cond, build))

    def arrive(kind, slot, cond=None, half=None):
        here = place(kind, slot, half)
        guarded(cond, lambda: copy_of(kind, here, slot, "core", 0, half).wait_recv())

    def forward(kind, slot, names, cond=None):
        for name in names:
            send(kind, slots[kind].at[slot[0], slot[1]], slot, name, cond)

    own = (fs, tp)
    orders = (("x", "y"), ("y", "x"))
    sources = (x_ref, g_ref)

    def crossed(kind, layer):
        if kind == 0:
            return (2 * layer + 1 - px, tp)
        return (2 * layer + px, tp_other)

    def lasts(kind, layer):
        if kind == 0:
            return ((2 * layer + px, tp_other), (2 * layer + 1 - px, tp_other))
        return ((2 * layer + 1 - px, tp), (2 * layer + 1 - px, tp_other))

    keep = [
        pltpu.make_async_copy(sources[kind], slots[kind].at[fs, tp], own_sem.at[kind])
        for kind in range(2)
    ]
    loads = [
        pltpu.make_async_copy(source, roots.at[which], own_sem.at[2 + which])
        for which, source in enumerate((rq_hbm, rf_hbm))
    ]
    for kind in range(2):
        send(kind, sources[kind], own, "up", has_up)
        send(kind, sources[kind], own, "down", has_down)
    for kind in range(2):
        send(kind, sources[kind], own, orders[kind][0])
    for kind in range(2):
        send(kind, sources[kind], own, orders[kind][1])
        send(kind, sources[kind], own, "core")
        keep[kind].start()
        loads[kind].start()

    def finals(stage):
        for layer, cond in stage:
            for kind in range(2):
                for slot in lasts(kind, layer):
                    arrive(kind, slot, cond)
                    forward(kind, slot, ("core",), cond)

    width = gs.shape[4]
    parts = gs.shape[1]
    chunk = s_ref.shape[1]
    steps = acc.shape[0] // chunk
    own_lanes = pl.ds(pl.multiple_of(tp * width, width), width)
    low = jnp.minimum(z, depth - 1 - z)

    def layer_of(turn):
        if turn == 0:
            return z
        near = z - (turn + 1) // 2 if turn % 2 == 1 else z + turn // 2
        far = jnp.where(2 * z < depth, turn, depth - 1 - turn)
        return jnp.where(turn <= 2 * low, near, far)

    def multiply(turn):
        layer = layer_of(turn)
        for across in range(2):
            for part in range(2):
                slot = (2 * layer + across, 2 * part + 1 - pc)
                for kind in range(2):
                    arrive(kind, slot, half=pc)
        for across in range(2):
            for part in range(parts):
                block_t = xs[2 * layer + across, part].T
                xt[part * span : (part + 1) * span, across * block : (across + 1) * block] = block_t
        first, final = turn == 0, turn == depth - 1
        both = pl.ds(2 * layer, 2)

        def step_body(step, total):
            rows = pl.ds(pl.multiple_of(step * chunk, chunk), chunk)
            for part in range(parts):
                cot = gs[both, part, pc].reshape(2 * block, width)
                piece = wide_dot(xt[rows, :], cot, ((1,), (0,)))
                lanes = slice(part * width, (part + 1) * width)
                if not first:
                    piece = piece + acc[rows, lanes]
                if final:
                    grad[rows, lanes] = to_bf16(piece)
                    total = total + jnp.sum(piece * piece, axis=0, keepdims=True)
                else:
                    acc[rows, lanes] = piece
            cot = gs[both, tp, 1 - pc].reshape(2 * block, width)
            piece = wide_dot(xt[rows, :], cot, ((1,), (0,)))
            if not first:
                piece = piece + other[rows, :]
            if final:
                owned[1 - pc, rows, :] = to_bf16(piece)
            else:
                other[rows, :] = piece
            return total

        return lax.fori_loop(0, steps, step_body, jnp.zeros((1, width), jnp.float32))

    def layers_at(distance):
        if distance == 0:
            return ((z, None),)
        return (
            (z - distance, z >= distance),
            (z + distance, z + distance < depth),
        )

    def along(distance):
        for onward, (layer, cond), more in zip(
            ("up", "down"), layers_at(distance), (has_up, has_down)
        ):
            for kind in range(2):
                slot = (2 * layer + px, tp)
                arrive(kind, slot, cond)
                if distance < depth - 1:
                    forward(kind, slot, (onward,), jnp.logical_and(cond, more))
                forward(kind, slot, orders[kind] + ("core",), cond)

    def across_pair(distance):
        for layer, cond in layers_at(distance):
            for kind in range(2):
                slot = crossed(kind, layer)
                arrive(kind, slot, cond)
                forward(kind, slot, (orders[kind][1], "core"), cond)

    for distance in range(1, depth):
        along(distance)
        if distance < depth - 1:
            across_pair(distance - 1)
    finals(layers_at(0))
    for kind in range(2):
        keep[kind].wait()
    multiply(0)
    across_pair(depth - 2)
    across_pair(depth - 1)
    for distance in range(1, depth - 1):
        finals(layers_at(distance))
        multiply(distance)
    finals(layers_at(depth - 1))
    total = multiply(depth - 1)

    tp_core = (fs, tp + 1 - 2 * pc)
    square = jnp.sum(total, axis=1, keepdims=True)
    norms[0] = jnp.broadcast_to(square, norms.shape[1:])
    swap_norm = pltpu.make_async_remote_copy(
        src_ref=norms.at[0], dst_ref=norms.at[1],
        send_sem=swap_sem.at[0], recv_sem=swap_sem.at[1],
        device_id=tp_core, device_id_type=MESH,
    )
    swap_rows = pltpu.make_async_remote_copy(
        src_ref=s_ref.at[pc], dst_ref=s_ref.at[pc],
        send_sem=swap_sem.at[2], recv_sem=swap_sem.at[3],
        device_id=tp_core, device_id_type=MESH,
    )
    take_rows = pltpu.make_async_remote_copy(
        src_ref=s_ref.at[1 - pc], dst_ref=s_ref.at[1 - pc],
        send_sem=swap_sem.at[2], recv_sem=swap_sem.at[3],
        device_id=tp_core, device_id_type=MESH,
    )
    size = float(grad.shape[0] * grad.shape[1])
    outer_scale = (1.0 - stat_decay) / grad.shape[1] * (size / (square + 1.0))
    mine = pl.ds(pl.multiple_of(fs * chunk, chunk), chunk)

    @pl.loop(0, steps)
    def _(step):
        rows = pl.ds(pl.multiple_of(step * chunk, chunk), chunk)
        outer = wide_dot(grad[mine, :], grad[rows, :], ((1,), (1,)))
        s_ref[pc, :, rows] = to_bf16(outer * outer_scale)
        owned[pc, rows, :] = grad[rows, own_lanes]

    swap_norm.start()
    heads = width // HEAD
    left[...] = jnp.zeros_like(left)
    kq_ref[...] = jnp.zeros_like(kq_ref)
    kf_ref[...] = jnp.zeros_like(kf_ref)
    swap_rows.start()
    for load in loads:
        load.wait()

    @pl.loop(0, steps)
    def _(step):
        rows = pl.ds(pl.multiple_of(step * chunk, chunk), chunk)
        for which, (root, col_ref) in enumerate(((roots.at[0], kq_ref), (roots.at[1], kf_ref))):
            part = owned[which, rows, :]
            left[which] += wide_dot(root[:, rows], part, ((1,), (0,)))
            for head in range(heads):
                piece = part[:, head * HEAD : (head + 1) * HEAD]
                col_ref[head] += wide_dot(piece, piece, ((0,), (0,)))

    swap_norm.wait()
    mine_sum, their_sum = norms[0, 0:1, 0:1], norms[1, 0:1, 0:1]
    sums = (
        jnp.where(pc == 0, mine_sum, their_sum),
        jnp.where(pc == 0, their_sum, mine_sum),
    )
    for which, (col_root, pre_ref, col_ref) in enumerate(
        ((cq_ref, pq_ref, kq_ref), (cf_ref, pf_ref, kf_ref))
    ):
        scale_twice = size / (sums[which] + 1.0)
        norm_scale = jnp.sqrt(scale_twice)
        for head in range(heads):
            lanes = slice(head * HEAD, (head + 1) * HEAD)
            col_ref[head] = col_ref[head] * ((1.0 - stat_decay) / grad.shape[0] * scale_twice)
            pre_ref[:, lanes] = norm_scale * wide_dot(
                to_bf16(left[which, :, lanes]), col_root[head], ((1,), (0,))
            )
    swap_rows.wait_send()
    take_rows.wait_recv()

    for cond, build in pending:
        guarded(cond, lambda build=build: build().wait_send())


def relayed_products(x, cots, query_root, forget_root, query_col_root, forget_col_root):
    shards, parts = lax.axis_size("fs"), lax.axis_size("tp")
    block, span = x.shape
    width = cots.shape[2]
    chunk, features = query_root.shape
    depth = shards // 2
    sends = 2 * (5 + 8 * (depth - 1) + 2 * (2 * depth - 1) + 2 * (2 * depth - 1))
    f32 = jnp.float32
    heads = query_col_root.shape
    vmem = pl.BlockSpec(memory_space=pltpu.VMEM)
    hbm = pl.BlockSpec(memory_space=pltpu.HBM)
    return pl.pallas_call(
        relay_kernel,
        out_shape=[
            jax.ShapeDtypeStruct((2, chunk, features), jnp.bfloat16),
            jax.ShapeDtypeStruct((chunk, width), f32),
            jax.ShapeDtypeStruct((chunk, width), f32),
            jax.ShapeDtypeStruct(heads, f32),
            jax.ShapeDtypeStruct(heads, f32),
        ],
        in_specs=[vmem, vmem, hbm, hbm, vmem, vmem],
        out_specs=[vmem] * 5,
        scratch_shapes=[
            pltpu.VMEM((shards, parts, block, span), jnp.bfloat16),
            pltpu.VMEM((shards, parts, 2, block, width), jnp.bfloat16),
            pltpu.VMEM((features, 2 * block), jnp.bfloat16),
            pltpu.VMEM((features, parts * width), f32),
            pltpu.VMEM((features, width), f32),
            pltpu.VMEM((features, parts * width), jnp.bfloat16),
            pltpu.VMEM((2, features, width), jnp.bfloat16),
            pltpu.VMEM((2, chunk, width), f32),
            pltpu.VMEM((2, 8, 128), f32),
            pltpu.VMEM((2, chunk, features), jnp.bfloat16),
            pltpu.SemaphoreType.DMA((4,)),
            pltpu.SemaphoreType.DMA((sends,)),
            pltpu.SemaphoreType.DMA((2, shards, parts)),
            pltpu.SemaphoreType.DMA((4,)),
        ],
        compiler_params=pltpu.CompilerParams(
            collective_id=0, has_side_effects=True, vmem_limit_bytes=61 * 1024 * 1024
        ),
    )(x, cots, query_root, forget_root, query_col_root, forget_col_root)


def pack_kernel(query_ref, forget_ref, pre_ref, bound_ref, out_ref):
    out_ref[0] = query_ref[...]
    sigma_gate = jax.nn.sigmoid(pre_ref[...].astype(jnp.float32))
    out_ref[1] = to_bf16(
        forget_ref[...].astype(jnp.float32)
        * (1.0 - bound_ref[...])
        * sigma_gate
        * (1.0 - sigma_gate)
    )


def packed_cotangents(query_grad, forget_grad, forget_pre, lower_bound):
    vmem = pl.BlockSpec(memory_space=pltpu.VMEM)
    return pl.pallas_call(
        pack_kernel,
        out_shape=jax.ShapeDtypeStruct((2,) + query_grad.shape, jnp.bfloat16),
        in_specs=[vmem] * 4,
        out_specs=vmem,
        compiler_params=pltpu.CompilerParams(vmem_limit_bytes=61 * 1024 * 1024),
    )(query_grad, forget_grad, forget_pre, lower_bound.reshape(1, -1))


def finish_kernel(outer_ref, *refs):
    pres, columns, weights, moments, rows, cols = (refs[2 * k : 2 * k + 2] for k in range(6))
    outs = refs[12:]
    for which in range(2):
        master_ref, copy_ref, step_ref, moment_ref, rows_ref, cols_ref = outs[which::2]
        precond = pres[which][...]
        moment_next = moment_decay * moments[which][...] + (1.0 - moment_decay) * precond
        update_step = moment_decay * moment_next + (1.0 - moment_decay) * precond
        master = weights[which][...] - learn_rate * update_step
        master_ref[...] = master
        copy_ref[...] = to_bf16(master)
        step_ref[...] = update_step
        moment_ref[...] = moment_next
        rows_ref[...] = stat_decay * rows[which][...] + outer_ref[which].astype(jnp.float32)
        cols_ref[...] = stat_decay * cols[which][...] + columns[which][...]


def finished(outers, pres, columns, weights, moments, rows, cols):
    f32, bf16 = jnp.float32, jnp.bfloat16
    chunk, width = weights[0].shape
    features = rows[0].shape[1]
    heads = cols[0].shape
    steps = 2
    tile = chunk // steps
    narrow = pl.BlockSpec((tile, width), lambda i: (i, 0))
    wide = pl.BlockSpec((tile, features), lambda i: (i, 0))
    head = pl.BlockSpec((heads[0], heads[1] // steps, heads[2]), lambda i: (0, i, 0))
    both = pl.BlockSpec((2, tile, features), lambda i: (0, i, 0))
    flat = lambda kind: [jax.ShapeDtypeStruct((chunk, width), kind)] * 2
    return pl.pallas_call(
        finish_kernel,
        grid=(steps,),
        out_shape=flat(f32)
        + flat(bf16)
        + flat(f32)
        + flat(f32)
        + [jax.ShapeDtypeStruct((chunk, features), f32)] * 2
        + [jax.ShapeDtypeStruct(heads, f32)] * 2,
        in_specs=[both] + [narrow] * 2 + [head] * 2 + [narrow] * 4 + [wide] * 2 + [head] * 2,
        out_specs=[narrow] * 8 + [wide] * 2 + [head] * 2,
        compiler_params=pltpu.CompilerParams(vmem_limit_bytes=61 * 1024 * 1024),
    )(outers, *pres, *columns, *weights, *moments, *rows, *cols)


def gather_plan(
    inputs,
    query_grad,
    forget_grad,
    forget_pre,
    lower_bound,
    query_weight,
    forget_weight,
    query_moment,
    forget_moment,
    query_rows,
    forget_rows,
    query_cols,
    forget_cols,
    query_row_root,
    forget_row_root,
    query_col_root,
    forget_col_root,
):
    outers, query_pre, forget_pre_out, query_column, forget_column = relayed_products(
        inputs,
        packed_cotangents(query_grad, forget_grad, forget_pre, lower_bound),
        query_row_root,
        forget_row_root,
        query_col_root,
        forget_col_root,
    )
    return tuple(
        finished(
            outers,
            (query_pre, forget_pre_out),
            (query_column, forget_column),
            (query_weight, forget_weight),
            (query_moment, forget_moment),
            (query_rows, forget_rows),
            (query_cols, forget_cols),
        )
    )


def on_device(*args):
    token_count = args[0].shape[0] * lax.axis_size("fs")
    feature_count = args[0].shape[1] * lax.axis_size("tp")
    paired = lax.axis_size("fs") % 2 == 0 and lax.axis_size("tp") == 4
    if paired and token_count <= feature_count:
        return gather_plan(*args)
    return reduce_plan(*args)


def solution(mesh):
    in_specs = (
        P("fs", "tp"),
        P("fs", "tp"),
        P("fs", "tp"),
        P("fs", "tp"),
        P("tp"),
        P("fs", "tp"),
        P("fs", "tp"),
        P("fs", "tp"),
        P("fs", "tp"),
        P("fs", None),
        P("fs", None),
        P("tp", None, None),
        P("tp", None, None),
        P("fs", None),
        P("fs", None),
        P("tp", None, None),
        P("tp", None, None),
    )
    out_specs = (
        P("fs", "tp"),
        P("fs", "tp"),
        P("fs", "tp"),
        P("fs", "tp"),
        P("fs", "tp"),
        P("fs", "tp"),
        P("fs", "tp"),
        P("fs", "tp"),
        P("fs", None),
        P("fs", None),
        P("tp", None, None),
        P("tp", None, None),
    )
    return jax.shard_map(
        on_device, mesh=mesh, in_specs=in_specs, out_specs=out_specs, check_vma=False
    )
```
